512 devices in a mesh: rep: 2 (over z_hi), fs: 32 (over z_lo, y), tp: 8 (over x, core).
Axes of the slice: x: 4, y: 4, z: 16 (z_hi: 2, z_lo: 8; z = z_hi * 8 + z_lo), core: 2. Of those that a mesh axis runs over, the one named last changes fastest.
Arguments:
- inputs: bfloat16 [24576, 2048], P(('rep', 'fs')), may hold values from -16 to 16
- w_up: bfloat16 [2048, 4096], P('fs', 'tp'), may hold values from -0.125 to 0.125
- w_down: bfloat16 [4096, 2048], P('tp', 'fs'), may hold values from -0.09375 to 0.09375
- cotangent: bfloat16 [24576, 2048], P(('rep', 'fs')), may hold values from -16 to 16
Outputs:
- d_inputs: bfloat16 [24576, 2048], P(('rep', 'fs'))
- d_w_up: float32 [2048, 4096], P('fs', 'tp')
The draws below stay inside these ranges and needn't reach their ends.
All inputs are finite; a program needn't handle non-finite values.
Results may differ from the reference program's by a relative error of at most 0.014.
Values may be sent and summed in bfloat16 or wider, within the bound.
No kernel may reach another device: no remote copies, remote signals or barrier semaphores. Data moves between devices by JAX's collectives and lax.ppermute only.
A program may use at most 64 MiB of HBM per device.

```python
import jax
import jax.numpy as jnp

D = 2048
FF = 4096
TOKENS = 24576
N_TP = 8


def strengthened(result, own_key, source, target, shards_of, factor):
    def block_of(axis_at):
        return (jnp.arange(result.shape[axis_at]) // (result.shape[axis_at] // shards_of)).reshape((-1,) + (1,) * (result.ndim - 1 - axis_at))

    near = jax.random.permutation(own_key, shards_of)[block_of(target)]
    other_side = (block_of(target) + shards_of // 2) % shards_of
    return jnp.where((block_of(source) == near) | (block_of(source) == other_side), factor * result, result)


def block_levels(key, extent, pieces, low, top_value):
    def one(dim, blocks):
        draws = jax.random.uniform(jax.random.fold_in(jax.random.fold_in(key, 6), dim), (blocks,), jnp.float32, low / len(pieces), top_value / len(pieces))
        return jnp.repeat(jnp.exp(draws), extent[dim] // blocks).reshape((-1,) + (1,) * (len(extent) - dim - 1))

    loudness = one(*pieces[0])
    for cut in pieces[1:]:
        loudness = loudness * one(*cut)
    return loudness


def normal_values(stream_key, extent, spread, most, split=(), kind=jnp.bfloat16):
    result = jax.random.normal(stream_key, extent, jnp.float32) * spread
    if len(split) > 0:
        result = block_levels(stream_key, extent, split, -0.22, 0.18) * result
    return jnp.clip(result, min=-most, max=most).astype(kind)


def gaussian_with(own_key, shape, deviation, reach, pieces, heavy, kind=jnp.bfloat16):
    drawn = deviation * jax.random.normal(own_key, shape, jnp.float32)
    if pieces:
        drawn = drawn * block_levels(own_key, shape, pieces, -0.22, 0.18)
    return jnp.clip(strengthened(drawn, jax.random.fold_in(own_key, 3), *heavy), -reach, reach).astype(kind)


def setup_inputs(seed: int = 0) -> dict:
    key_of = jax.random.split(jax.random.key(seed), 5)
    inputs = gaussian_with(key_of[0], (TOKENS, D), 1.0, 16.0, ((0, 64),), (0, 1, 64, 4.0))
    w_up = normal_values(key_of[1], (D, FF), D ** -0.5, 0.125, ((0, 32), (1, 8)))
    w_down = normal_values(key_of[2], (FF, D), FF ** -0.5, 0.09375, ((0, 8), (1, 32)))
    cotangent = gaussian_with(key_of[3], (TOKENS, D), 1.0, 16.0, ((0, 64),), (0, 1, 64, 4.0))
    return {"inputs": inputs, "w_up": w_up, "w_down": w_down, "cotangent": cotangent}


def reference(inputs, w_up, w_down, cotangent):
    preact = jnp.dot(inputs, w_up, preferred_element_type=jnp.float32)
    grad_hidden = jnp.dot(cotangent, w_down.T, preferred_element_type=jnp.float32)
    grad_pre = (2.0 * jnp.maximum(preact, 0.0) * grad_hidden).astype(jnp.bfloat16)
    tp_cols = FF // N_TP
    accumulated = jnp.zeros(inputs.shape, jnp.float32)
    for shard_index in range(N_TP):
        lower = shard_index * tp_cols
        partial_sum = jnp.dot(grad_pre[:, lower:lower + tp_cols], w_up[:, lower:lower + tp_cols].T,
                              preferred_element_type=jnp.float32).astype(jnp.bfloat16)
        accumulated = accumulated + partial_sum.astype(jnp.float32)
    d_inputs = accumulated.astype(jnp.bfloat16)
    d_w_up = jnp.dot(inputs.T, grad_pre, preferred_element_type=jnp.float32)
    return d_inputs, d_w_up
```

```python
import functools

import jax
import jax.numpy as jnp
from jax import lax
from jax.experimental import pallas as pl
from jax.experimental.pallas import tpu as pltpu
from jax.sharding import Mesh
from jax.sharding import PartitionSpec as P

FS = ("fs_0", "fs_1")
REP_FS = ("rep", "fs_0", "fs_1")
CHUNKS = 1

BF = jnp.bfloat16
F32 = jnp.float32


def exchange(parts, axes):
    return lax.all_to_all(parts, axes, split_axis=0, concat_axis=0, tiled=True)


def copies_over(value, axes):
    return exchange(jnp.broadcast_to(value, (lax.axis_size(axes), *value.shape)), axes)


def block_kernel(first, last, x_ref, c_ref, w_ref, *refs):
    prev_ref, refs = (None, refs) if first else (refs[0], refs[1:])
    part_ref, dw_ref, pre_acc, hid_acc = refs
    n_y, n_z, two_rows, _ = w_ref.shape
    rows = two_rows // 2
    width = n_y * rows

    def up(z):
        return jnp.concatenate([w_ref[y, z, :rows] for y in range(n_y)], axis=0)

    def down(z):
        return jnp.concatenate([w_ref[y, z, rows:] for y in range(n_y)], axis=0)

    for z in range(n_z):
        cols = slice(z * width, (z + 1) * width)
        pre = jnp.dot(x_ref[:, cols], up(z), preferred_element_type=F32)
        hid = jnp.dot(c_ref[:, cols], down(z), preferred_element_type=F32)
        if z == 0:
            pre_acc[...] = pre
            hid_acc[...] = hid
        else:
            pre_acc[...] += pre
            hid_acc[...] += hid
    grad = (2.0 * jnp.maximum(pre_acc[...], 0.0) * hid_acc[...]).astype(BF)
    for z in range(n_z):
        cols = slice(z * width, (z + 1) * width)
        dw = lax.dot_general(
            x_ref[:, cols], grad, (((0,), (0,)), ((), ())), preferred_element_type=F32
        ).astype(BF)
        for y in range(n_y):
            dw_ref[y, z] = dw[y * rows : (y + 1) * rows]
        part = lax.dot_general(
            grad, up(z), (((1,), (1,)), ((), ())), preferred_element_type=F32
        )
        if not first:
            part = part + prev_ref[:, cols]
        part_ref[:, cols] = part.astype(part_ref.dtype)


def block_grads(x, c, w, prev, last):
    n_y, n_z, two_rows, h = w.shape
    first = prev is None
    args = (x, c, w) if first else (x, c, w, prev)
    vm = pl.BlockSpec(memory_space=pltpu.VMEM)
    return pl.pallas_call(
        functools.partial(block_kernel, first, last),
        out_shape=(
            jax.ShapeDtypeStruct(x.shape, BF if last else F32),
            jax.ShapeDtypeStruct((n_y, n_z, two_rows // 2, h), BF),
        ),
        in_specs=[vm] * len(args),
        out_specs=(vm, vm),
        scratch_shapes=[pltpu.VMEM((x.shape[0], h), F32)] * 2,
        cost_estimate=pl.CostEstimate(
            flops=8 * x.shape[0] * x.shape[1] * h,
            bytes_accessed=2 * (3 * x.size + 3 * x.shape[1] * h),
            transcendentals=0,
        ),
    )(*args)


def per_device(inputs, w_up, w_down, cotangent):
    rows, hidden = w_up.shape
    both = jnp.concatenate([w_up, w_down.T], axis=0)
    h = hidden // CHUNKS
    prev = None
    grads = []
    for k in range(CHUNKS):
        own = both[:, k * h : (k + 1) * h]
        along_z = copies_over(own, "fs_0")
        whole = copies_over(along_z, "fs_1")
        prev, dw = block_grads(inputs, cotangent, whole, prev, k == CHUNKS - 1)
        summed = exchange(dw, "fs_1").astype(F32).sum(0).astype(BF)
        n_z = summed.shape[0]
        halves = jnp.moveaxis(summed.reshape(n_z, 2, rows // 2, h), 1, 0)
        mine = exchange(halves.reshape(2 * n_z, rows // 2, h), ("rep", "fs_0"))
        mine = mine.astype(F32).sum(0).astype(BF)
        grads.append(copies_over(mine, "rep").reshape(rows, h))
    d_w_up = jnp.concatenate(grads, axis=1).astype(F32)
    n_tp = lax.axis_size("tp")
    tokens, width = prev.shape
    pieces = exchange(prev.reshape(n_tp, tokens // n_tp, width), "tp")
    own_rows = pieces.astype(F32).sum(0).astype(BF)
    d_inputs = copies_over(own_rows, "tp").reshape(tokens, width)
    return (d_inputs, d_w_up)


def solution(mesh):
    split = Mesh(
        mesh.devices.reshape(mesh.shape["rep"], 8, 4, mesh.shape["tp"]),
        ("rep", "fs_0", "fs_1", "tp"),
    )
    placed = (P(REP_FS, None), P(FS, "tp"), P("tp", FS), P(REP_FS, None))
    return jax.shard_map(
        per_device,
        mesh=split,
        in_specs=placed,
        out_specs=(P(REP_FS, None), P(FS, "tp")),
        check_vma=False,
    )
```

```python
import jax
import jax.numpy as jnp
from jax import lax
from jax.experimental import pallas as pl
from jax.experimental.pallas import tpu as pltpu
from jax.sharding import Mesh
from jax.sharding import PartitionSpec as P

FS = ("zh", "zl", "y")
REP_FS = ("rep", "zh", "zl", "y")
Z = ("rep", "zh", "zl")
TP = ("x", "core")
N_Z = 8
N_Y = 4

BF = jnp.bfloat16
F32 = jnp.float32
SHIFTS = (0, 1, -1, 2, -2, 3, -3, 4)


def exchange(parts, axes):
    return lax.all_to_all(parts, axes, split_axis=0, concat_axis=0, tiled=True)


def shifted(value, axes, step):
    n = lax.axis_size(axes)
    return lax.ppermute(value, axes, [(i, (i + step) % n) for i in range(n)])


def swapped(value, axes, partner):
    n = lax.axis_size(axes)
    return lax.ppermute(value, axes, [(i, partner(i)) for i in range(n)])


def block_kernel(
    x_ref, c_ref, own_ref, prev_ref, next_ref, far_a_ref, far_b_ref,
    keep_ref, give_ref, dw_ref, up, down, pre_acc, hid_acc, grad, sems,
):
    me_y = lax.axis_index("y")
    me_z = lax.axis_index("zh") * 4 + lax.axis_index("zl")
    core = lax.axis_index("core")
    rows = own_ref.shape[1] // 2
    width = N_Y * rows
    half = N_Z // 2

    def source(dist, r):
        if dist == 0:
            return own_ref.at[r]
        if dist == 1:
            return prev_ref.at[r]
        if dist == -1:
            return next_ref.at[r]
        return far_a_ref.at[r] if r < half else far_b_ref.at[r - half]

    copies = []
    starts = []
    for r, shift in enumerate(SHIFTS):
        z = lax.rem(me_z - shift + 2 * N_Z, N_Z)
        starts.append(pl.multiple_of(z * width, width))
        group = []
        for k, dist in enumerate((0, 1, -1, 2)):
            y = lax.rem(me_y - dist + 2 * N_Y, N_Y)
            at = pl.ds(pl.multiple_of(z * width + y * rows, rows), rows)
            for part, dst in enumerate((up, down)):
                copy = pltpu.make_async_copy(
                    source(dist, r).at[pl.ds(part * rows, rows)],
                    dst.at[at],
                    sems.at[r, k, part],
                )
                copy.start()
                group.append(copy)
        copies.append(group)
    for r in range(N_Z):
        for copy in copies[r]:
            copy.wait()
        at = pl.ds(starts[r], width)
        pre = jnp.dot(x_ref[:, at], up[at, :], preferred_element_type=F32)
        hid = jnp.dot(c_ref[:, at], down[at, :], preferred_element_type=F32)
        if r == 0:
            pre_acc[...] = pre
            hid_acc[...] = hid
        else:
            pre_acc[...] += pre
            hid_acc[...] += hid
    grad[...] = (2.0 * jnp.maximum(pre_acc[...], 0.0) * hid_acc[...]).astype(BF)
    for z in range(N_Z):
        cols = slice(z * width, (z + 1) * width)
        dw = lax.dot_general(
            x_ref[:, cols], grad[...], (((0,), (0,)), ((), ())),
            preferred_element_type=F32,
        ).astype(BF)
        for y in range(N_Y):
            dw_ref[y, z % 4, z // 4] = dw[y * rows : (y + 1) * rows]
    tokens = x_ref.shape[0] // 2
    for out, which in ((give_ref, 1 - core), (keep_ref, core)):
        mine = grad[pl.ds(pl.multiple_of(which * tokens, tokens), tokens), :]
        for z in range(N_Z):
            cols = slice(z * width, (z + 1) * width)
            out[:, cols] = lax.dot_general(
                mine, up[cols, :], (((1,), (1,)), ((), ())),
                preferred_element_type=F32,
            ).astype(BF)


def block_grads(x, c, own, prev, following, far_a, far_b):
    tokens, width = x.shape
    rows, h = own.shape[1] // 2, own.shape[2]
    vm = pl.BlockSpec(memory_space=pltpu.VMEM)
    any_ = pl.BlockSpec(memory_space=pl.ANY)
    half = jax.ShapeDtypeStruct((tokens // 2, width), BF)
    return pl.pallas_call(
        block_kernel,
        out_shape=(half, half, jax.ShapeDtypeStruct((N_Y, 4, 2, rows, h), BF)),
        in_specs=[vm] * 2 + [any_] * 5,
        out_specs=(vm, vm, vm),
        scratch_shapes=[
            pltpu.VMEM((width, h), BF),
            pltpu.VMEM((width, h), BF),
            pltpu.VMEM((tokens, h), F32),
            pltpu.VMEM((tokens, h), F32),
            pltpu.VMEM((tokens, h), BF),
            pltpu.SemaphoreType.DMA((N_Z, N_Y, 2)),
        ],
        cost_estimate=pl.CostEstimate(
            flops=8 * tokens * width * h,
            bytes_accessed=2 * (3 * tokens * width + 3 * width * h),
            transcendentals=0,
        ),
    )(x, c, own, prev, following, far_a, far_b)


def total(a, b):
    return (a.astype(F32) + b.astype(F32)).astype(BF)


def per_device(inputs, w_up, w_down, cotangent):
    rows, h = w_up.shape
    down = w_down.T
    both = jnp.concatenate([w_up, down], axis=0)
    blocks = [both] + [shifted(both, Z, s) for s in SHIFTS[1:-1]]
    blocks.append(
        jnp.concatenate([shifted(w_up, Z, 4), shifted(down, Z, -4)], axis=0)
    )
    own = jnp.stack(blocks)
    prev = shifted(own, "y", 1)
    following = shifted(own, "y", -1)
    far_a = shifted(prev[: N_Z // 2], "y", 1)
    far_b = shifted(following[N_Z // 2 :], "y", -1)
    keep, give, dw = block_grads(
        inputs, cotangent, own, prev, following, far_a, far_b
    )

    over_core = total(keep, swapped(give, "core", lambda i: 1 - i))
    over_pair = total(over_core, swapped(over_core, "x", lambda i: i ^ 1))
    mine = total(over_pair, swapped(over_pair, "x", lambda i: 3 - i))
    other = swapped(mine, "core", lambda i: 1 - i)
    first = lax.axis_index("core") == 0
    d_inputs = jnp.concatenate(
        [jnp.where(first, mine, other), jnp.where(first, other, mine)], axis=0
    )

    over_y = exchange(dw, "y").astype(F32).sum(0).astype(BF)
    over_near = exchange(over_y, "zl").astype(F32).sum(0).astype(BF)
    to_far = jnp.broadcast_to(over_near, (2, *over_near.shape))
    d_w_up = exchange(to_far.reshape(4, rows, h), ("rep", "zh")).astype(F32).sum(0)
    return (d_inputs, d_w_up)


def solution(mesh):
    split = Mesh(
        mesh.devices.reshape(2, 2, 4, N_Y, 4, 2),
        ("rep", "zh", "zl", "y", "x", "core"),
    )
    placed = (P(REP_FS, None), P(FS, TP), P(TP, FS), P(REP_FS, None))
    return jax.shard_map(
        per_device,
        mesh=split,
        in_specs=placed,
        out_specs=(P(REP_FS, None), P(FS, TP)),
        check_vma=False,
    )
```

```python
import jax
import jax.numpy as jnp
from jax import lax
from jax.experimental import pallas as pl
from jax.experimental.pallas import tpu as pltpu
from jax.sharding import Mesh
from jax.sharding import PartitionSpec as P

FS = ("zh", "zl", "y")
REP_FS = ("rep", "zh", "zl", "y")
Z = ("rep", "zh", "zl")
TP = ("x", "core")
N_Z = 8
N_Y = 4

BF = jnp.bfloat16
F32 = jnp.float32
NEAR = (0, 1, -1)
FAR = (2, -2, 3, -3, 4)


def exchange(parts, axes):
    return lax.all_to_all(parts, axes, split_axis=0, concat_axis=0, tiled=True)


def copies_over(value, axes):
    n = lax.axis_size(axes)
    copies = jnp.broadcast_to(value, (n, *value.shape))
    return exchange(copies, axes)


def shifted(value, axes, step):
    n = lax.axis_size(axes)
    return lax.ppermute(value, axes, [(i, (i + step) % n) for i in range(n)])


def swapped(value, axes, partner):
    n = lax.axis_size(axes)
    return lax.ppermute(value, axes, [(i, partner(i)) for i in range(n)])


def z_blocks(near_ref, far_ref):
    me = lax.axis_index("zh") * 4 + lax.axis_index("zl")
    for ref, shifts in ((near_ref, NEAR), (far_ref, FAR)):
        for k, shift in enumerate(shifts):
            yield ref, k, lax.rem(me - shift + 2 * N_Z, N_Z)


def rows_of(ref, k, part):
    rows = ref.shape[2] // 2
    at = slice(part * rows, (part + 1) * rows)
    return jnp.concatenate([ref[y, k, at] for y in range(N_Y)], axis=0)


def weight_kernel(x_ref, c_ref, near_ref, far_ref, grad_ref, dw_ref, pre_acc, hid_acc):
    rows = near_ref.shape[2] // 2
    width = N_Y * rows
    for n, (ref, k, z) in enumerate(z_blocks(near_ref, far_ref)):
        at = pl.ds(pl.multiple_of(z * width, width), width)
        pre = jnp.dot(x_ref[:, at], rows_of(ref, k, 0), preferred_element_type=F32)
        hid = jnp.dot(c_ref[:, at], rows_of(ref, k, 1), preferred_element_type=F32)
        if n == 0:
            pre_acc[...] = pre
            hid_acc[...] = hid
        else:
            pre_acc[...] += pre
            hid_acc[...] += hid
    grad_ref[...] = (2.0 * jnp.maximum(pre_acc[...], 0.0) * hid_acc[...]).astype(BF)
    for z in range(N_Z):
        dw = lax.dot_general(
            x_ref[:, z * width : (z + 1) * width], grad_ref[...],
            (((0,), (0,)), ((), ())), preferred_element_type=F32,
        ).astype(BF)
        for y in range(N_Y):
            dw_ref[y, z % 4, z // 4] = dw[y * rows : (y + 1) * rows]


def input_kernel(grad_ref, near_ref, far_ref, keep_ref, give_ref):
    core = lax.axis_index("core")
    tokens = keep_ref.shape[0]
    width = N_Y * near_ref.shape[2] // 2
    for out, which in ((give_ref, 1 - core), (keep_ref, core)):
        mine = grad_ref[pl.ds(pl.multiple_of(which * tokens, tokens), tokens), :]
        for ref, k, z in z_blocks(near_ref, far_ref):
            out[:, pl.ds(pl.multiple_of(z * width, width), width)] = lax.dot_general(
                mine, rows_of(ref, k, 0), (((1,), (1,)), ((), ())),
                preferred_element_type=F32,
            ).astype(BF)


def call(kernel, outs, args, flops, scratch=()):
    vm = pl.BlockSpec(memory_space=pltpu.VMEM)
    return pl.pallas_call(
        kernel,
        out_shape=tuple(jax.ShapeDtypeStruct(s, BF) for s in outs),
        in_specs=[vm] * len(args),
        out_specs=(vm,) * len(outs),
        scratch_shapes=scratch,
        cost_estimate=pl.CostEstimate(
            flops=flops,
            bytes_accessed=2 * sum(a.size for a in args),
            transcendentals=0,
        ),
    )(*args)


def total(a, b):
    return (a.astype(F32) + b.astype(F32)).astype(BF)


def per_device(inputs, w_up, w_down, cotangent):
    rows, h = w_up.shape
    tokens, width = inputs.shape
    own = jnp.concatenate([w_up, w_down.T], axis=0)
    back = [own]
    ahead = [own]
    for _ in range(3):
        back.append(shifted(back[-1], Z, 1))
        ahead.append(shifted(ahead[-1], Z, -1))
    last = jnp.concatenate(
        [shifted(back[3][:rows], Z, 1), shifted(ahead[3][rows:], Z, -1)], axis=0
    )
    near = copies_over(jnp.stack([own, back[1], ahead[1]]), "y")
    far = copies_over(jnp.stack([back[2], ahead[2], back[3], ahead[3], last]), "y")
    flops = 4 * tokens * width * h
    grad, dw = call(
        weight_kernel,
        [(tokens, h), (N_Y, 4, 2, rows, h)],
        (inputs, cotangent, near, far),
        3 * flops // 2,
        [pltpu.VMEM((tokens, h), F32)] * 2,
    )
    keep, give = call(
        input_kernel, [(tokens // 2, width)] * 2, (grad, near, far), flops // 2
    )

    over_core = total(keep, swapped(give, "core", lambda i: 1 - i))
    over_pair = total(over_core, swapped(over_core, "x", lambda i: i ^ 1))
    mine = total(over_pair, swapped(over_pair, "x", lambda i: 3 - i))
    other = swapped(mine, "core", lambda i: 1 - i)
    first = lax.axis_index("core") == 0
    d_inputs = jnp.concatenate(
        [jnp.where(first, mine, other), jnp.where(first, other, mine)], axis=0
    )

    over_y = exchange(dw, "y").astype(F32).sum(0).astype(BF)
    over_near = exchange(over_y, "zl").astype(F32).sum(0).astype(BF)
    to_far = jnp.broadcast_to(over_near, (2, *over_near.shape))
    d_w_up = exchange(to_far.reshape(4, rows, h), ("rep", "zh")).astype(F32).sum(0)
    return (d_inputs, d_w_up)


def solution(mesh):
    split = Mesh(
        mesh.devices.reshape(2, 2, 4, N_Y, 4, 2),
        ("rep", "zh", "zl", "y", "x", "core"),
    )
    placed = (P(REP_FS, None), P(FS, TP), P(TP, FS), P(REP_FS, None))
    return jax.shard_map(
        per_device,
        mesh=split,
        in_specs=placed,
        out_specs=(P(REP_FS, None), P(FS, TP)),
        check_vma=False,
    )
```

```python
import jax
import jax.numpy as jnp
from jax import lax
from jax.experimental import pallas as pl
from jax.experimental.pallas import tpu as pltpu
from jax.sharding import Mesh
from jax.sharding import PartitionSpec as P


FS = ("zh", "zl", "y")
REP_FS = ("rep", "zh", "zl", "y")
Z = ("rep", "zh", "zl")
TP = ("x", "core")
N_Z = 8
N_Y = 4

BF = jnp.bfloat16
F32 = jnp.float32
NEAR = (0, 1, -1, 2, -2)
FAR = (3, -3, 4)


def exchange(parts, axes):
    return lax.all_to_all(parts, axes, split_axis=0, concat_axis=0, tiled=True)


def copies_over(value, axes):
    n = lax.axis_size(axes)
    copies = jnp.broadcast_to(value, (n, *value.shape))
    return exchange(copies, axes)


def shifted(value, axes, step):
    n = lax.axis_size(axes)
    return lax.ppermute(value, axes, [(i, (i + step) % n) for i in range(n)])


def swapped(value, axes, partner):
    n = lax.axis_size(axes)
    return lax.ppermute(value, axes, [(i, partner(i)) for i in range(n)])


def z_blocks(*groups):
    me = lax.axis_index("zh") * 4 + lax.axis_index("zl")
    for ref, shifts in groups:
        for k, shift in enumerate(shifts):
            yield ref, k, lax.rem(me - shift + 2 * N_Z, N_Z)


def rows_of(ref, k, part):
    rows = ref.shape[2] // 2
    at = slice(part * rows, (part + 1) * rows)
    return jnp.concatenate([ref[y, k, at] for y in range(N_Y)], axis=0)


def add_products(x_ref, c_ref, ref, shifts, pre_acc, hid_acc, fresh):
    width = N_Y * ref.shape[2] // 2
    for ref, k, z in z_blocks((ref, shifts)):
        at = pl.ds(pl.multiple_of(z * width, width), width)
        pre = jnp.dot(x_ref[:, at], rows_of(ref, k, 0), preferred_element_type=F32)
        hid = jnp.dot(c_ref[:, at], rows_of(ref, k, 1), preferred_element_type=F32)
        if fresh and k == 0:
            pre_acc[...] = pre
            hid_acc[...] = hid
        else:
            pre_acc[...] += pre
            hid_acc[...] += hid


def near_kernel(x_ref, c_ref, near_ref, pre_ref, hid_ref):
    add_products(x_ref, c_ref, near_ref, NEAR, pre_ref, hid_ref, True)


def weight_kernel(
    x_ref, c_ref, far_ref, pre_ref, hid_ref, grad_ref, dw_ref, pre_acc, hid_acc
):
    rows = far_ref.shape[2] // 2
    width = N_Y * rows
    pre_acc[...] = pre_ref[...]
    hid_acc[...] = hid_ref[...]
    add_products(x_ref, c_ref, far_ref, FAR, pre_acc, hid_acc, False)
    grad_ref[...] = (2.0 * jnp.maximum(pre_acc[...], 0.0) * hid_acc[...]).astype(BF)
    for z in range(N_Z):
        dw = lax.dot_general(
            x_ref[:, z * width : (z + 1) * width], grad_ref[...],
            (((0,), (0,)), ((), ())), preferred_element_type=F32,
        ).astype(BF)
        for y in range(N_Y):
            dw_ref[y, z % 4, z // 4] = dw[y * rows : (y + 1) * rows]


def input_kernel(grad_ref, near_ref, far_ref, keep_ref, give_ref):
    core = lax.axis_index("core")
    tokens = keep_ref.shape[0]
    width = N_Y * near_ref.shape[2] // 2
    for out, which in ((give_ref, 1 - core), (keep_ref, core)):
        mine = grad_ref[pl.ds(pl.multiple_of(which * tokens, tokens), tokens), :]
        for ref, k, z in z_blocks((near_ref, NEAR), (far_ref, FAR)):
            out[:, pl.ds(pl.multiple_of(z * width, width), width)] = lax.dot_general(
                mine, rows_of(ref, k, 0), (((1,), (1,)), ((), ())),
                preferred_element_type=F32,
            ).astype(BF)


def call(kernel, outs, args, flops, scratch=(), dtype=BF):
    vm = pl.BlockSpec(memory_space=pltpu.VMEM)
    return pl.pallas_call(
        kernel,
        out_shape=tuple(jax.ShapeDtypeStruct(s, dtype) for s in outs),
        in_specs=[vm] * len(args),
        out_specs=(vm,) * len(outs),
        scratch_shapes=scratch,
        cost_estimate=pl.CostEstimate(
            flops=flops,
            bytes_accessed=2 * sum(a.size for a in args),
            transcendentals=0,
        ),
    )(*args)


def total(a, b):
    return (a.astype(F32) + b.astype(F32)).astype(BF)


def per_device(inputs, w_up, w_down, cotangent):
    rows, h = w_up.shape
    tokens, width = inputs.shape
    own = jnp.concatenate([w_up, w_down.T], axis=0)
    back = [shifted(own, Z, 1)]
    ahead = [shifted(own, Z, -1)]
    back.append(shifted(own, Z, 2))
    ahead.append(shifted(own, Z, -2))
    near = jnp.stack([own, back[0], ahead[0], back[1], ahead[1]])
    near = copies_over(near, "y")
    back = shifted(jnp.concatenate([back[0], back[1][:rows]], axis=0), Z, 2)
    ahead = shifted(jnp.concatenate([ahead[0], ahead[1][rows:]], axis=0), Z, -2)
    last = jnp.concatenate([back[2 * rows :], ahead[2 * rows :]], axis=0)
    far = jnp.stack([back[: 2 * rows], ahead[: 2 * rows], last])
    far = copies_over(far, "y")
    unit = tokens * width * h // 2
    pre, hid = call(
        near_kernel, [(tokens, h)] * 2, (inputs, cotangent, near), 5 * unit, dtype=F32
    )
    grad, dw = call(
        weight_kernel,
        [(tokens, h), (N_Y, 4, 2, rows, h)],
        (inputs, cotangent, far, pre, hid),
        7 * unit,
        [pltpu.VMEM((tokens, h), F32)] * 2,
    )
    keep, give = call(
        input_kernel, [(tokens // 2, width)] * 2, (grad, near, far), 4 * unit
    )

    over_core = total(keep, swapped(give, "core", lambda i: 1 - i))
    over_pair = total(over_core, swapped(over_core, "x", lambda i: i ^ 1))
    mine = total(over_pair, swapped(over_pair, "x", lambda i: 3 - i))
    other = swapped(mine, "core", lambda i: 1 - i)
    first = lax.axis_index("core") == 0
    d_inputs = jnp.concatenate(
        [jnp.where(first, mine, other), jnp.where(first, other, mine)], axis=0
    )

    by_y = exchange(dw, "y")
    over_y = by_y.astype(F32).sum(0).astype(BF)
    over_near = exchange(over_y, "zl").astype(F32).sum(0).astype(BF)
    to_far = jnp.broadcast_to(over_near, (2, *over_near.shape))
    d_w_up = exchange(to_far.reshape(4, rows, h), ("rep", "zh")).astype(F32).sum(0)
    return (d_inputs, d_w_up)


def solution(mesh):
    split = Mesh(
        mesh.devices.reshape(2, 2, 4, N_Y, 4, 2),
        ("rep", "zh", "zl", "y", "x", "core"),
    )
    placed = (P(REP_FS, None), P(FS, TP), P(TP, FS), P(REP_FS, None))
    return jax.shard_map(
        per_device,
        mesh=split,
        in_specs=placed,
        out_specs=(P(REP_FS, None), P(FS, TP)),
        check_vma=False,
    )
```

```python
import jax
import jax.numpy as jnp
from jax import lax
from jax.experimental import pallas as pl
from jax.experimental.pallas import tpu as pltpu
from jax.sharding import Mesh
from jax.sharding import PartitionSpec as P


FS = ("zh", "zl", "y")
REP_FS = ("rep", "zh", "zl", "y")
Z = ("rep", "zh", "zl")
TP = ("x", "core")
N_Z = 8
N_Y = 4

BF = jnp.bfloat16
F32 = jnp.float32
NEAR = (0, 1, -1)
FAR = (2, -2, 3, -3, 4)


def exchange(parts, axes):
    return lax.all_to_all(parts, axes, split_axis=0, concat_axis=0, tiled=True)


def copies_over(value, axes):
    n = lax.axis_size(axes)
    copies = jnp.broadcast_to(value, (n, *value.shape))
    return exchange(copies, axes)


def shifted(value, axes, step):
    n = lax.axis_size(axes)
    return lax.ppermute(value, axes, [(i, (i + step) % n) for i in range(n)])


def swapped(value, axes, partner):
    n = lax.axis_size(axes)
    return lax.ppermute(value, axes, [(i, partner(i)) for i in range(n)])


def z_blocks(*groups):
    me = lax.axis_index("zh") * 4 + lax.axis_index("zl")
    for ref, shifts in groups:
        for k, shift in enumerate(shifts):
            yield ref, k, lax.rem(me - shift + 2 * N_Z, N_Z)


def rows_of(ref, k, part):
    rows = ref.shape[2] // 2
    at = slice(part * rows, (part + 1) * rows)
    return jnp.concatenate([ref[y, k, at] for y in range(N_Y)], axis=0)


def add_products(x_ref, c_ref, ref, shifts, pre_acc, hid_acc, fresh):
    width = N_Y * ref.shape[2] // 2
    for ref, k, z in z_blocks((ref, shifts)):
        at = pl.ds(pl.multiple_of(z * width, width), width)
        pre = jnp.dot(x_ref[:, at], rows_of(ref, k, 0), preferred_element_type=F32)
        hid = jnp.dot(c_ref[:, at], rows_of(ref, k, 1), preferred_element_type=F32)
        if fresh and k == 0:
            pre_acc[...] = pre
            hid_acc[...] = hid
        else:
            pre_acc[...] += pre
            hid_acc[...] += hid


def near_kernel(x_ref, c_ref, near_ref, pre_ref, hid_ref):
    add_products(x_ref, c_ref, near_ref, NEAR, pre_ref, hid_ref, True)


def weight_kernel(
    x_ref, c_ref, far_ref, pre_ref, hid_ref, grad_ref, dw_ref, pre_acc, hid_acc
):
    rows = far_ref.shape[2] // 2
    width = N_Y * rows
    pre_acc[...] = pre_ref[...]
    hid_acc[...] = hid_ref[...]
    add_products(x_ref, c_ref, far_ref, FAR, pre_acc, hid_acc, False)
    grad_ref[...] = (2.0 * jnp.maximum(pre_acc[...], 0.0) * hid_acc[...]).astype(BF)
    for z in range(N_Z):
        dw = lax.dot_general(
            x_ref[:, z * width : (z + 1) * width], grad_ref[...],
            (((0,), (0,)), ((), ())), preferred_element_type=F32,
        ).astype(BF)
        for y in range(N_Y):
            dw_ref[y, z % 4, z // 4] = dw[y * rows : (y + 1) * rows]


def input_kernel(grad_ref, near_ref, far_ref, keep_ref, give_ref):
    core = lax.axis_index("core")
    tokens = keep_ref.shape[0]
    width = N_Y * near_ref.shape[2] // 2
    for out, which in ((give_ref, 1 - core), (keep_ref, core)):
        mine = grad_ref[pl.ds(pl.multiple_of(which * tokens, tokens), tokens), :]
        for ref, k, z in z_blocks((near_ref, NEAR), (far_ref, FAR)):
            out[:, pl.ds(pl.multiple_of(z * width, width), width)] = lax.dot_general(
                mine, rows_of(ref, k, 0), (((1,), (1,)), ((), ())),
                preferred_element_type=F32,
            ).astype(BF)


def call(kernel, outs, args, flops, scratch=(), dtype=BF):
    vm = pl.BlockSpec(memory_space=pltpu.VMEM)
    return pl.pallas_call(
        kernel,
        out_shape=tuple(jax.ShapeDtypeStruct(s, dtype) for s in outs),
        in_specs=[vm] * len(args),
        out_specs=(vm,) * len(outs),
        scratch_shapes=scratch,
        cost_estimate=pl.CostEstimate(
            flops=flops,
            bytes_accessed=2 * sum(a.size for a in args),
            transcendentals=0,
        ),
    )(*args)


def total(a, b):
    return (a.astype(F32) + b.astype(F32)).astype(BF)


def per_device(inputs, w_up, w_down, cotangent):
    rows, h = w_up.shape
    tokens, width = inputs.shape
    own = jnp.concatenate([w_up, w_down.T], axis=0)
    back = [own]
    ahead = [own]
    for _ in range(3):
        back.append(shifted(back[-1], Z, 1))
        ahead.append(shifted(ahead[-1], Z, -1))
    last = jnp.concatenate(
        [shifted(back[3][:rows], Z, 1), shifted(ahead[3][rows:], Z, -1)], axis=0
    )
    near = copies_over(jnp.stack([own, back[1], ahead[1]]), "y")
    far = copies_over(jnp.stack([back[2], ahead[2], back[3], ahead[3], last]), "y")
    unit = tokens * width * h // 2
    pre, hid = call(
        near_kernel, [(tokens, h)] * 2, (inputs, cotangent, near), 3 * unit, dtype=F32
    )
    grad, dw = call(
        weight_kernel,
        [(tokens, h), (N_Y, 4, 2, rows, h)],
        (inputs, cotangent, far, pre, hid),
        9 * unit,
        [pltpu.VMEM((tokens, h), F32)] * 2,
    )
    keep, give = call(
        input_kernel, [(tokens // 2, width)] * 2, (grad, near, far), 4 * unit
    )

    over_core = total(keep, swapped(give, "core", lambda i: 1 - i))
    step = swapped(over_core, "x", lambda i: i ^ 1)
    over_pair = total(over_core, step)
    step = swapped(over_pair, "x", lambda i: 3 - i)
    mine = total(over_pair, step)
    other = swapped(mine, "core", lambda i: 1 - i)
    first = lax.axis_index("core") == 0
    d_inputs = jnp.concatenate(
        [jnp.where(first, mine, other), jnp.where(first, other, mine)], axis=0
    )

    by_y = exchange(dw, "y")
    over_y = by_y.astype(F32).sum(0).astype(BF)
    by_near = exchange(over_y, "zl")
    over_near = by_near.astype(F32).sum(0).astype(BF)
    to_far = jnp.broadcast_to(over_near, (2, *over_near.shape)).reshape(4, rows, h)
    by_far = exchange(to_far, ("rep", "zh"))
    return (d_inputs, by_far.astype(F32).sum(0))


def solution(mesh):
    split = Mesh(
        mesh.devices.reshape(2, 2, 4, N_Y, 4, 2),
        ("rep", "zh", "zl", "y", "x", "core"),
    )
    placed = (P(REP_FS, None), P(FS, TP), P(TP, FS), P(REP_FS, None))
    return jax.shard_map(
        per_device,
        mesh=split,
        in_specs=placed,
        out_specs=(P(REP_FS, None), P(FS, TP)),
        check_vma=False,
    )
```

```python
import jax
import jax.numpy as jnp
from jax import lax
from jax.experimental import pallas as pl
from jax.experimental.pallas import tpu as pltpu
from jax.sharding import Mesh
from jax.sharding import PartitionSpec as P


FS = ("zh", "zl", "y")
REP_FS = ("rep", "zh", "zl", "y")
Z = ("rep", "zh", "zl")
TP = ("x", "core")
N_Z = 8
N_Y = 4

BF = jnp.bfloat16
F32 = jnp.float32
NEAR = (0, 1, -1)
FAR = (2, -2, 3, -3, 4)


def exchange(parts, axes):
    return lax.all_to_all(parts, axes, split_axis=0, concat_axis=0, tiled=True)


def copies_over(value, axes):
    n = lax.axis_size(axes)
    copies = jnp.broadcast_to(value, (n, *value.shape))
    return exchange(copies, axes)


def shifted(value, axes, step):
    n = lax.axis_size(axes)
    return lax.ppermute(value, axes, [(i, (i + step) % n) for i in range(n)])


def swapped(value, axes, partner):
    n = lax.axis_size(axes)
    return lax.ppermute(value, axes, [(i, partner(i)) for i in range(n)])


def z_blocks(*groups):
    me = lax.axis_index("zh") * 4 + lax.axis_index("zl")
    for ref, shifts in groups:
        for k, shift in enumerate(shifts):
            yield ref, k, lax.rem(me - shift + 2 * N_Z, N_Z)


def rows_of(ref, k, part):
    rows = ref.shape[2] // 2
    at = slice(part * rows, (part + 1) * rows)
    return jnp.concatenate([ref[y, k, at] for y in range(N_Y)], axis=0)


def add_products(x_ref, c_ref, ref, shifts, pre_acc, hid_acc, fresh):
    width = N_Y * ref.shape[2] // 2
    for ref, k, z in z_blocks((ref, shifts)):
        at = pl.ds(pl.multiple_of(z * width, width), width)
        pre = jnp.dot(x_ref[:, at], rows_of(ref, k, 0), preferred_element_type=F32)
        hid = jnp.dot(c_ref[:, at], rows_of(ref, k, 1), preferred_element_type=F32)
        if fresh and k == 0:
            pre_acc[...] = pre
            hid_acc[...] = hid
        else:
            pre_acc[...] += pre
            hid_acc[...] += hid


def near_kernel(x_ref, c_ref, near_ref, pre_ref, hid_ref):
    add_products(x_ref, c_ref, near_ref, NEAR, pre_ref, hid_ref, True)


def far_copies(plus, minus, dsts, sems):
    me = lax.axis_index("y")
    rows = plus[0].shape[0] // 5
    width = N_Y * rows
    copies = []
    for n in range(len(FAR)):
        group = []
        for part, dst in enumerate(dsts):
            if n < 4:
                refs, piece = (plus, minus)[n % 2], n // 2 * 2 + part
            else:
                refs, piece = (plus, minus)[part], 4
            for k, dist in enumerate((0, 1, -1, 2)):
                y = lax.rem(me - dist + 2 * N_Y, N_Y)
                at = pl.multiple_of(n * width + y * rows, rows)
                copy = pltpu.make_async_copy(
                    refs[k].at[pl.ds(piece * rows, rows)],
                    dst.at[pl.ds(at, rows)],
                    sems.at[n, part, k],
                )
                copy.start()
                group.append(copy)
        copies.append(group)
    return copies


def weight_kernel(x_hbm, c_hbm, pre_hbm, hid_hbm, *refs):
    plus, minus = refs[0:4], refs[4:8]
    grad_ref, dw_hbm, x, c, up, down, pre_acc, hid_acc, dw, sems, far_sems, out_sems = (
        refs[8:]
    )
    width = dw.shape[1] * dw.shape[2]
    first = [
        pltpu.make_async_copy(src, dst, sems.at[k])
        for k, (src, dst) in enumerate(
            ((x_hbm, x), (pre_hbm, pre_acc), (hid_hbm, hid_acc))
        )
    ]
    for copy in first:
        copy.start()
    places = []
    c_copies = []
    for n, (_, _, z) in enumerate(z_blocks((None, FAR))):
        at = pl.ds(pl.multiple_of(z * width, width), width)
        copy = pltpu.make_async_copy(c_hbm.at[:, at], c.at[n], sems.at[3 + n])
        copy.start()
        places.append(at)
        c_copies.append(copy)
    blocks = far_copies(plus, minus, (up, down), far_sems)
    for copy in first:
        copy.wait()
    for n, at in enumerate(places):
        for copy in (c_copies[n], *blocks[n]):
            copy.wait()
        mine = slice(n * width, (n + 1) * width)
        pre_acc[...] += jnp.dot(x[:, at], up[mine], preferred_element_type=F32)
        hid_acc[...] += jnp.dot(c[n], down[mine], preferred_element_type=F32)
    grad_ref[...] = (2.0 * jnp.maximum(pre_acc[...], 0.0) * hid_acc[...]).astype(BF)
    out = []
    for z in range(N_Z):
        product = lax.dot_general(
            x[:, z * width : (z + 1) * width], grad_ref[...],
            (((0,), (0,)), ((), ())), preferred_element_type=F32,
        ).astype(BF)
        dw[z] = product.reshape(dw.shape[1:])
        copy = pltpu.make_async_copy(
            dw.at[z], dw_hbm.at[:, z % 4, z // 4], out_sems.at[z]
        )
        copy.start()
        out.append(copy)
    for copy in out:
        copy.wait()


def input_kernel(grad_ref, near_ref, *refs):
    plus, minus = refs[0:4], refs[4:8]
    keep_ref, give_ref, up, sems = refs[8:]
    core = lax.axis_index("core")
    tokens = keep_ref.shape[0]
    width = N_Y * near_ref.shape[2] // 2
    copies = far_copies(plus, minus, (up,), sems)
    for group in copies:
        for copy in group:
            copy.wait()
    for out, which in ((give_ref, 1 - core), (keep_ref, core)):
        mine = grad_ref[pl.ds(pl.multiple_of(which * tokens, tokens), tokens), :]
        for ref, k, z in z_blocks((near_ref, NEAR), (None, FAR)):
            if ref is None:
                block = up[k * width : (k + 1) * width]
            else:
                block = rows_of(ref, k, 0)
            out[:, pl.ds(pl.multiple_of(z * width, width), width)] = lax.dot_general(
                mine, block, (((1,), (1,)), ((), ())), preferred_element_type=F32
            ).astype(BF)


def call(kernel, outs, args, flops, in_hbm, scratch=(), dtype=BF, out_hbm=()):
    vm = pl.BlockSpec(memory_space=pltpu.VMEM)
    hbm = pl.BlockSpec(memory_space=pl.ANY)
    return pl.pallas_call(
        kernel,
        out_shape=tuple(jax.ShapeDtypeStruct(s, dtype) for s in outs),
        in_specs=[hbm if k in in_hbm else vm for k in range(len(args))],
        out_specs=tuple(hbm if k in out_hbm else vm for k in range(len(outs))),
        scratch_shapes=scratch,
        cost_estimate=pl.CostEstimate(
            flops=flops,
            bytes_accessed=2 * sum(a.size for a in args),
            transcendentals=0,
        ),
    )(*args)


def total(a, b):
    return (a.astype(F32) + b.astype(F32)).astype(BF)


def per_device(inputs, w_up, w_down, cotangent):
    rows, h = w_up.shape
    tokens, width = inputs.shape
    own = jnp.concatenate([w_up, w_down.T], axis=0)
    back = [own]
    ahead = [own]
    for _ in range(3):
        back.append(shifted(back[-1], Z, 1))
        ahead.append(shifted(ahead[-1], Z, -1))
    plus_last = shifted(back[3][:rows], Z, 1)
    minus_last = shifted(ahead[3][rows:], Z, -1)
    near = copies_over(jnp.stack([own, back[1], ahead[1]]), "y")
    plus = [jnp.concatenate([back[2], back[3], plus_last], axis=0)]
    minus = [jnp.concatenate([ahead[2], ahead[3], minus_last], axis=0)]
    plus.append(shifted(plus[0], "y", 1))
    minus_after = shifted(minus[0], "y", -1)
    minus.append(shifted(minus[0], "y", 1))
    plus.append(shifted(plus[0], "y", -1))
    minus.append(minus_after)
    plus.append(shifted(plus[1], "y", 1))
    minus.append(shifted(minus_after, "y", -1))
    unit = tokens * width * h // 2
    part = N_Y * rows
    pre, hid = call(
        near_kernel,
        [(tokens, h)] * 2,
        (inputs, cotangent, near),
        3 * unit,
        (),
        dtype=F32,
    )
    grad, dw = call(
        weight_kernel,
        [(tokens, h), (N_Y, 4, 2, rows, h)],
        (inputs, cotangent, pre, hid, *plus, *minus),
        9 * unit,
        range(12),
        [
            pltpu.VMEM((tokens, width), BF),
            pltpu.VMEM((len(FAR), tokens, part), BF),
            pltpu.VMEM((len(FAR) * part, h), BF),
            pltpu.VMEM((len(FAR) * part, h), BF),
            pltpu.VMEM((tokens, h), F32),
            pltpu.VMEM((tokens, h), F32),
            pltpu.VMEM((N_Z, N_Y, rows, h), BF),
            pltpu.SemaphoreType.DMA((3 + len(FAR),)),
            pltpu.SemaphoreType.DMA((len(FAR), 2, N_Y)),
            pltpu.SemaphoreType.DMA((N_Z,)),
        ],
        out_hbm=(1,),
    )
    keep, give = call(
        input_kernel,
        [(tokens // 2, width)] * 2,
        (grad, near, *plus, *minus),
        4 * unit,
        range(2, 10),
        [
            pltpu.VMEM((len(FAR) * part, h), BF),
            pltpu.SemaphoreType.DMA((len(FAR), 1, N_Y)),
        ],
    )

    over_core = total(keep, swapped(give, "core", lambda i: 1 - i))
    step = swapped(over_core, "x", lambda i: i ^ 1)
    over_pair = total(over_core, step)
    step = swapped(over_pair, "x", lambda i: 3 - i)
    mine = total(over_pair, step)
    other = swapped(mine, "core", lambda i: 1 - i)
    first = lax.axis_index("core") == 0
    d_inputs = jnp.concatenate(
        [jnp.where(first, mine, other), jnp.where(first, other, mine)], axis=0
    )

    by_y = exchange(dw, "y")
    over_y = by_y.astype(F32).sum(0).astype(BF)
    by_near = exchange(over_y, "zl")
    over_near = by_near.astype(F32).sum(0).astype(BF)
    to_far = jnp.broadcast_to(over_near, (2, *over_near.shape)).reshape(4, rows, h)
    by_far = exchange(to_far, ("rep", "zh"))
    return (d_inputs, by_far.astype(F32).sum(0))


def solution(mesh):
    split = Mesh(
        mesh.devices.reshape(2, 2, 4, N_Y, 4, 2),
        ("rep", "zh", "zl", "y", "x", "core"),
    )
    placed = (P(REP_FS, None), P(FS, TP), P(TP, FS), P(REP_FS, None))
    return jax.shard_map(
        per_device,
        mesh=split,
        in_specs=placed,
        out_specs=(P(REP_FS, None), P(FS, TP)),
        check_vma=False,
    )
```

```python
import jax
import jax.numpy as jnp
from jax import lax
from jax.experimental import pallas as pl
from jax.experimental.pallas import tpu as pltpu
from jax.sharding import Mesh
from jax.sharding import PartitionSpec as P


FS = ("zh", "zl", "y")
REP_FS = ("rep", "zh", "zl", "y")
Z = ("rep", "zh", "zl")
TP = ("x", "core")
N_Z = 8
N_Y = 4

BF = jnp.bfloat16
F32 = jnp.float32
NEAR = (0, 1, -1)
FAR = (2, -2, 3, -3, 4)


def exchange(parts, axes):
    return lax.all_to_all(parts, axes, split_axis=0, concat_axis=0, tiled=True)


def copies_over(value, axes):
    n = lax.axis_size(axes)
    copies = jnp.broadcast_to(value, (n, *value.shape))
    return exchange(copies, axes)


def shifted(value, axes, step):
    n = lax.axis_size(axes)
    return lax.ppermute(value, axes, [(i, (i + step) % n) for i in range(n)])


def swapped(value, axes, partner):
    n = lax.axis_size(axes)
    return lax.ppermute(value, axes, [(i, partner(i)) for i in range(n)])


def z_blocks(*groups):
    me = lax.axis_index("zh") * 4 + lax.axis_index("zl")
    for ref, shifts in groups:
        for k, shift in enumerate(shifts):
            yield ref, k, lax.rem(me - shift + 2 * N_Z, N_Z)


def rows_of(ref, k, part):
    rows = ref.shape[2] // 2
    at = slice(part * rows, (part + 1) * rows)
    return jnp.concatenate([ref[y, k, at] for y in range(N_Y)], axis=0)


def add_products(x_ref, c_ref, ref, shifts, pre_acc, hid_acc, fresh):
    width = N_Y * ref.shape[2] // 2
    for ref, k, z in z_blocks((ref, shifts)):
        at = pl.ds(pl.multiple_of(z * width, width), width)
        pre = jnp.dot(x_ref[:, at], rows_of(ref, k, 0), preferred_element_type=F32)
        hid = jnp.dot(c_ref[:, at], rows_of(ref, k, 1), preferred_element_type=F32)
        if fresh and k == 0:
            pre_acc[...] = pre
            hid_acc[...] = hid
        else:
            pre_acc[...] += pre
            hid_acc[...] += hid


def near_kernel(x_ref, c_ref, near_ref, pre_ref, hid_ref):
    add_products(x_ref, c_ref, near_ref, NEAR, pre_ref, hid_ref, True)


def far_copies(plus, minus, dsts, sems):
    me = lax.axis_index("y")
    rows = minus[0].shape[0] // 4
    width = N_Y * rows
    copies = []
    for n in range(len(FAR)):
        group = []
        refs = (plus, minus)[n % 2]
        for part, dst in enumerate(dsts):
            piece = n // 2 * 2 + part
            for k, dist in enumerate((0, 1, -1, 2)):
                y = lax.rem(me - dist + 2 * N_Y, N_Y)
                at = pl.multiple_of(n * width + y * rows, rows)
                copy = pltpu.make_async_copy(
                    refs[k].at[pl.ds(piece * rows, rows)],
                    dst.at[pl.ds(at, rows)],
                    sems.at[n, part, k],
                )
                group.append(copy)
        copies.append(group)
    return copies


def weight_kernel(x_hbm, c_hbm, pre_hbm, hid_hbm, *refs):
    plus, minus = refs[0:4], refs[4:8]
    grad_ref, dw_hbm, x, c, up, down, pre_near, hid_near, pre_acc, hid_acc = refs[8:18]
    dw, x_sems, c_sems, sums_sems, far_sems, out_sems = refs[18:]
    width = dw.shape[1] * dw.shape[2]
    blocks = far_copies(plus, minus, (up, down), far_sems)
    sums = [
        pltpu.make_async_copy(pre_hbm, pre_near, sums_sems.at[0]),
        pltpu.make_async_copy(hid_hbm, hid_near, sums_sems.at[1]),
    ]
    places = [z for _, _, z in z_blocks((None, FAR), (None, NEAR))]
    x_copies = []
    for n, z in enumerate(places):
        at = pl.ds(pl.multiple_of(z * width, width), width)
        x_copies.append(pltpu.make_async_copy(x_hbm.at[:, at], x.at[n], x_sems.at[n]))
        x_copies[n].start()
        if n < len(FAR):
            copy = pltpu.make_async_copy(c_hbm.at[:, at], c.at[n], c_sems.at[n])
            blocks[n].append(copy)
            for copy in blocks[n]:
                copy.start()
        if n == len(FAR) - 1:
            for copy in sums:
                copy.start()
    for n in range(len(FAR)):
        for copy in (x_copies[n], *blocks[n]):
            copy.wait()
        mine = slice(n * width, (n + 1) * width)
        pre = jnp.dot(x[n], up[mine], preferred_element_type=F32)
        hid = jnp.dot(c[n], down[mine], preferred_element_type=F32)
        if n == 0:
            pre_acc[...] = pre
            hid_acc[...] = hid
        else:
            pre_acc[...] += pre
            hid_acc[...] += hid
    for copy in sums:
        copy.wait()
    pre = pre_acc[...] + pre_near[...]
    grad_ref[...] = (2.0 * jnp.maximum(pre, 0.0) * (hid_acc[...] + hid_near[...])).astype(BF)
    out = []
    for n, z in enumerate(places):
        if n >= len(FAR):
            x_copies[n].wait()
        product = lax.dot_general(
            x[n], grad_ref[...], (((0,), (0,)), ((), ())), preferred_element_type=F32
        ).astype(BF)
        dw[n] = product.reshape(dw.shape[1:])
        copy = pltpu.make_async_copy(
            dw.at[n], dw_hbm.at[:, lax.rem(z, 4), lax.div(z, 4)], out_sems.at[n]
        )
        copy.start()
        out.append(copy)
    for copy in out:
        copy.wait()


def input_kernel(grad_ref, near_ref, *refs):
    plus, minus = refs[0:4], refs[4:8]
    keep_ref, give_ref, up, sems = refs[8:]
    core = lax.axis_index("core")
    tokens = keep_ref.shape[0]
    width = N_Y * near_ref.shape[2] // 2
    copies = far_copies(plus, minus, (up,), sems)
    for group in copies:
        for copy in group:
            copy.start()
    for group in copies:
        for copy in group:
            copy.wait()
    for out, which in ((give_ref, 1 - core), (keep_ref, core)):
        mine = grad_ref[pl.ds(pl.multiple_of(which * tokens, tokens), tokens), :]
        for ref, k, z in z_blocks((near_ref, NEAR), (None, FAR)):
            if ref is None:
                block = up[k * width : (k + 1) * width]
            else:
                block = rows_of(ref, k, 0)
            out[:, pl.ds(pl.multiple_of(z * width, width), width)] = lax.dot_general(
                mine, block, (((1,), (1,)), ((), ())), preferred_element_type=F32
            ).astype(BF)


def call(kernel, outs, args, flops, in_hbm, scratch=(), dtype=BF, out_hbm=()):
    vm = pl.BlockSpec(memory_space=pltpu.VMEM)
    hbm = pl.BlockSpec(memory_space=pl.ANY)
    return pl.pallas_call(
        kernel,
        out_shape=tuple(jax.ShapeDtypeStruct(s, dtype) for s in outs),
        in_specs=[hbm if k in in_hbm else vm for k in range(len(args))],
        out_specs=tuple(hbm if k in out_hbm else vm for k in range(len(outs))),
        scratch_shapes=scratch,
        cost_estimate=pl.CostEstimate(
            flops=flops,
            bytes_accessed=2 * sum(a.size for a in args),
            transcendentals=0,
        ),
    )(*args)


def total(a, b):
    return (a.astype(F32) + b.astype(F32)).astype(BF)


def per_device(inputs, w_up, w_down, cotangent):
    rows, h = w_up.shape
    tokens, width = inputs.shape
    own = jnp.concatenate([w_up, w_down.T], axis=0)
    back = [own]
    ahead = [own]
    for _ in range(3):
        back.append(shifted(back[-1], Z, 1))
        ahead.append(shifted(ahead[-1], Z, -1))
    last = shifted(back[3], Z, 1)
    near = copies_over(jnp.stack([own, back[1], ahead[1]]), "y")
    plus = [jnp.concatenate([back[2], back[3], last], axis=0)]
    minus = [jnp.concatenate([ahead[2], ahead[3]], axis=0)]
    plus.append(shifted(plus[0], "y", 1))
    minus_after = shifted(minus[0], "y", -1)
    minus.append(shifted(minus[0], "y", 1))
    plus.append(shifted(plus[0], "y", -1))
    minus.append(minus_after)
    plus.append(shifted(plus[1], "y", 1))
    minus.append(shifted(minus_after, "y", -1))
    unit = tokens * width * h // 2
    part = N_Y * rows
    pre, hid = call(
        near_kernel,
        [(tokens, h)] * 2,
        (inputs, cotangent, near),
        3 * unit,
        (),
        dtype=F32,
    )
    grad, dw = call(
        weight_kernel,
        [(tokens, h), (N_Y, 4, 2, rows, h)],
        (inputs, cotangent, pre, hid, *plus, *minus),
        9 * unit,
        range(12),
        [
            pltpu.VMEM((N_Z, tokens, part), BF),
            pltpu.VMEM((len(FAR), tokens, part), BF),
            pltpu.VMEM((len(FAR) * part, h), BF),
            pltpu.VMEM((len(FAR) * part, h), BF),
            *[pltpu.VMEM((tokens, h), F32)] * 4,
            pltpu.VMEM((N_Z, N_Y, rows, h), BF),
            pltpu.SemaphoreType.DMA((N_Z,)),
            pltpu.SemaphoreType.DMA((len(FAR),)),
            pltpu.SemaphoreType.DMA((2,)),
            pltpu.SemaphoreType.DMA((len(FAR), 2, N_Y)),
            pltpu.SemaphoreType.DMA((N_Z,)),
        ],
        out_hbm=(1,),
    )
    keep, give = call(
        input_kernel,
        [(tokens // 2, width)] * 2,
        (grad, near, *plus, *minus),
        4 * unit,
        range(2, 10),
        [
            pltpu.VMEM((len(FAR) * part, h), BF),
            pltpu.SemaphoreType.DMA((len(FAR), 1, N_Y)),
        ],
    )

    over_core = total(keep, swapped(give, "core", lambda i: 1 - i))
    step = swapped(over_core, "x", lambda i: i ^ 1)
    over_pair = total(over_core, step)
    step = swapped(over_pair, "x", lambda i: 3 - i)
    mine = total(over_pair, step)
    other = swapped(mine, "core", lambda i: 1 - i)
    first = lax.axis_index("core") == 0
    d_inputs = jnp.concatenate(
        [jnp.where(first, mine, other), jnp.where(first, other, mine)], axis=0
    )

    by_y = exchange(dw, "y")
    over_y = by_y.astype(F32).sum(0).astype(BF)
    by_near = exchange(over_y, "zl")
    over_near = by_near.astype(F32).sum(0).astype(BF)
    to_far = jnp.broadcast_to(over_near, (2, *over_near.shape)).reshape(4, rows, h)
    by_far = exchange(to_far, ("rep", "zh"))
    return (d_inputs, by_far.astype(F32).sum(0))


def solution(mesh):
    split = Mesh(
        mesh.devices.reshape(2, 2, 4, N_Y, 4, 2),
        ("rep", "zh", "zl", "y", "x", "core"),
    )
    placed = (P(REP_FS, None), P(FS, TP), P(TP, FS), P(REP_FS, None))
    return jax.shard_map(
        per_device,
        mesh=split,
        in_specs=placed,
        out_specs=(P(REP_FS, None), P(FS, TP)),
        check_vma=False,
    )
```

```python
import jax
import jax.numpy as jnp
from jax import lax
from jax.experimental import pallas as pl
from jax.experimental.pallas import tpu as pltpu
from jax.sharding import Mesh
from jax.sharding import PartitionSpec as P


FS = ("zh", "zl", "y")
REP_FS = ("rep", "zh", "zl", "y")
Z = ("rep", "zh", "zl")
TP = ("x", "core")
N_Z = 8
N_Y = 4

BF = jnp.bfloat16
F32 = jnp.float32
NEAR = (0, 1, -1)
FAR = (2, -2, 3, -3, 4)


def exchange(parts, axes):
    return lax.all_to_all(parts, axes, split_axis=0, concat_axis=0, tiled=True)


def copies_over(value, axes):
    n = lax.axis_size(axes)
    copies = jnp.broadcast_to(value, (n, *value.shape))
    return exchange(copies, axes)


def shifted(value, axes, step):
    n = lax.axis_size(axes)
    return lax.ppermute(value, axes, [(i, (i + step) % n) for i in range(n)])


def swapped(value, axes, partner):
    n = lax.axis_size(axes)
    return lax.ppermute(value, axes, [(i, partner(i)) for i in range(n)])


def near_z(k):
    me = lax.axis_index("zh") * 4 + lax.axis_index("zl")
    step = jnp.where(k == 0, 0, jnp.where(k == 1, 1, -1))
    return lax.rem(me - step + 2 * N_Z, N_Z)


def far_z(n):
    me = lax.axis_index("zh") * 4 + lax.axis_index("zl")
    step = (2 + lax.div(n, 2)) * (1 - 2 * lax.rem(n, 2))
    return lax.rem(me - step + 2 * N_Z, N_Z)


def block(index, width):
    return pl.ds(pl.multiple_of(index * width, width), width)


def near_rows(ref, k, part):
    rows = ref.shape[2] // 2
    at = slice(part * rows, (part + 1) * rows)
    return jnp.concatenate([ref[y, k, at] for y in range(N_Y)], axis=0)


def near_kernel(x_ref, c_ref, near_ref, pre_ref, hid_ref):
    width = N_Y * near_ref.shape[2] // 2
    pre_ref[...] = jnp.zeros_like(pre_ref)
    hid_ref[...] = jnp.zeros_like(hid_ref)

    @pl.loop(0, len(NEAR))
    def _(k):
        at = block(near_z(k), width)
        up, down = near_rows(near_ref, k, 0), near_rows(near_ref, k, 1)
        pre_ref[...] += jnp.dot(x_ref[:, at], up, preferred_element_type=F32)
        hid_ref[...] += jnp.dot(c_ref[:, at], down, preferred_element_type=F32)


def far_copies(n, plus, minus, dsts, sems):
    me = lax.axis_index("y")
    rows = plus[0].shape[0] // 5
    copies = []
    for part, dst in enumerate(dsts):
        if n < 4:
            refs, piece = (plus, minus)[n % 2], n // 2 * 2 + part
        else:
            refs, piece = (plus, minus)[part], 4
        for k, dist in enumerate((0, 1, -1, 2)):
            y = lax.rem(me - dist + 2 * N_Y, N_Y)
            at = pl.multiple_of(n * N_Y * rows + y * rows, rows)
            src = refs[k].at[pl.ds(piece * rows, rows)]
            copies.append(
                pltpu.make_async_copy(src, dst.at[pl.ds(at, rows)], sems.at[n, part, k])
            )
    return copies


def wait_far(n, like, dsts, sems):
    rows = like.shape[0] // 5
    for part, dst in enumerate(dsts):
        for k in range(N_Y):
            at = block(n * N_Y + k, rows)
            pltpu.make_async_copy(
                like.at[pl.ds(0, rows)], dst.at[at], sems.at[n, part, k]
            ).wait()


def weight_kernel(x_hbm, c_hbm, pre_hbm, hid_hbm, *refs):
    plus, minus = refs[0:4], refs[4:8]
    grad_ref, dw_hbm, x, c, up, down, pre_near, hid_near, pre_acc, hid_acc = refs[8:18]
    dw, x_sems, c_sems, sums_sems, far_sems, out_sems = refs[18:]
    width = dw.shape[1] * dw.shape[2]

    def x_copy(z):
        at = block(z, width)
        return pltpu.make_async_copy(x_hbm.at[:, at], x.at[:, at], x_sems.at[z])

    def c_copy(n):
        at = block(far_z(n), width)
        return pltpu.make_async_copy(c_hbm.at[:, at], c.at[n], c_sems.at[n])

    def out_copy(z):
        to = dw_hbm.at[:, lax.rem(z, 4), lax.div(z, 4)]
        return pltpu.make_async_copy(dw.at[z], to, out_sems.at[z])

    for n in range(len(FAR)):
        x_copy(far_z(n)).start()
        c_copy(n).start()
        for copy in far_copies(n, plus, minus, (up, down), far_sems):
            copy.start()
    sums = [
        pltpu.make_async_copy(pre_hbm, pre_near, sums_sems.at[0]),
        pltpu.make_async_copy(hid_hbm, hid_near, sums_sems.at[1]),
    ]
    for copy in sums:
        copy.start()
    for k in range(len(NEAR)):
        x_copy(near_z(k)).start()
    pre_acc[...] = jnp.zeros_like(pre_acc)
    hid_acc[...] = jnp.zeros_like(hid_acc)

    @pl.loop(0, len(FAR))
    def _(n):
        z = far_z(n)
        x_copy(z).wait()
        c_copy(n).wait()
        wait_far(n, plus[0], (up, down), far_sems)
        mine = block(n, width)
        cols = x[:, block(z, width)]
        pre_acc[...] += jnp.dot(cols, up[mine, :], preferred_element_type=F32)
        hid_acc[...] += jnp.dot(c[n], down[mine, :], preferred_element_type=F32)

    for copy in sums:
        copy.wait()
    pre = pre_acc[...] + pre_near[...]
    hid = hid_acc[...] + hid_near[...]
    grad_ref[...] = (2.0 * jnp.maximum(pre, 0.0) * hid).astype(BF)
    for k in range(len(NEAR)):
        x_copy(near_z(k)).wait()

    @pl.loop(0, N_Z)
    def _(z):
        product = lax.dot_general(
            x[:, block(z, width)], grad_ref[...], (((0,), (0,)), ((), ())),
            preferred_element_type=F32,
        ).astype(BF)
        dw[z] = product.reshape(dw.shape[1:])
        out_copy(z).start()

    for z in range(N_Z):
        out_copy(z).wait()


def input_kernel(grad_ref, near_ref, *refs):
    plus, minus = refs[0:4], refs[4:8]
    keep_ref, give_ref, up, sems = refs[8:]
    core = lax.axis_index("core")
    tokens = keep_ref.shape[0]
    width = N_Y * near_ref.shape[2] // 2
    for n in range(len(FAR)):
        for copy in far_copies(n, plus, minus, (up,), sems):
            copy.start()

    def product(out, which, z, rows):
        mine = grad_ref[block(which, tokens), :]
        out[:, block(z, width)] = lax.dot_general(
            mine, rows, (((1,), (1,)), ((), ())), preferred_element_type=F32
        ).astype(BF)

    @pl.loop(0, len(NEAR))
    def _(k):
        rows = near_rows(near_ref, k, 0)
        product(give_ref, 1 - core, near_z(k), rows)
        product(keep_ref, core, near_z(k), rows)

    @pl.loop(0, len(FAR))
    def _(n):
        wait_far(n, plus[0], (up,), sems)
        rows = up[block(n, width), :]
        product(give_ref, 1 - core, far_z(n), rows)
        product(keep_ref, core, far_z(n), rows)


def call(kernel, outs, args, flops, in_hbm, scratch=(), dtype=BF, out_hbm=()):
    vm = pl.BlockSpec(memory_space=pltpu.VMEM)
    hbm = pl.BlockSpec(memory_space=pl.ANY)
    return pl.pallas_call(
        kernel,
        out_shape=tuple(jax.ShapeDtypeStruct(s, dtype) for s in outs),
        in_specs=[hbm if k in in_hbm else vm for k in range(len(args))],
        out_specs=tuple(hbm if k in out_hbm else vm for k in range(len(outs))),
        scratch_shapes=scratch,
        cost_estimate=pl.CostEstimate(
            flops=flops,
            bytes_accessed=2 * sum(a.size for a in args),
            transcendentals=0,
        ),
    )(*args)


def total(a, b):
    return (a.astype(F32) + b.astype(F32)).astype(BF)


def per_device(inputs, w_up, w_down, cotangent):
    rows, h = w_up.shape
    tokens, width = inputs.shape
    own = jnp.concatenate([w_up, w_down.T], axis=0)
    back = [own]
    ahead = [own]
    for _ in range(3):
        back.append(shifted(back[-1], Z, 1))
        ahead.append(shifted(ahead[-1], Z, -1))
    plus_last = shifted(back[3][:rows], Z, 1)
    minus_last = shifted(ahead[3][rows:], Z, -1)
    near = copies_over(jnp.stack([own, back[1], ahead[1]]), "y")
    plus = [jnp.concatenate([back[2], back[3], plus_last], axis=0)]
    minus = [jnp.concatenate([ahead[2], ahead[3], minus_last], axis=0)]
    plus.append(shifted(plus[0], "y", 1))
    minus_after = shifted(minus[0], "y", -1)
    minus.append(shifted(minus[0], "y", 1))
    plus.append(shifted(plus[0], "y", -1))
    minus.append(minus_after)
    plus.append(shifted(plus[1], "y", 1))
    minus.append(shifted(minus_after, "y", -1))
    unit = tokens * width * h // 2
    part = N_Y * rows
    pre, hid = call(
        near_kernel,
        [(tokens, h)] * 2,
        (inputs, cotangent, near),
        3 * unit,
        (),
        dtype=F32,
    )
    grad, dw = call(
        weight_kernel,
        [(tokens, h), (N_Y, 4, 2, rows, h)],
        (inputs, cotangent, pre, hid, *plus, *minus),
        9 * unit,
        range(12),
        [
            pltpu.VMEM((tokens, width), BF),
            pltpu.VMEM((len(FAR), tokens, part), BF),
            pltpu.VMEM((len(FAR) * part, h), BF),
            pltpu.VMEM((len(FAR) * part, h), BF),
            *[pltpu.VMEM((tokens, h), F32)] * 4,
            pltpu.VMEM((N_Z, N_Y, rows, h), BF),
            pltpu.SemaphoreType.DMA((N_Z,)),
            pltpu.SemaphoreType.DMA((len(FAR),)),
            pltpu.SemaphoreType.DMA((2,)),
            pltpu.SemaphoreType.DMA((len(FAR), 2, N_Y)),
            pltpu.SemaphoreType.DMA((N_Z,)),
        ],
        out_hbm=(1,),
    )
    keep, give = call(
        input_kernel,
        [(tokens // 2, width)] * 2,
        (grad, near, *plus, *minus),
        4 * unit,
        range(2, 10),
        [
            pltpu.VMEM((len(FAR) * part, h), BF),
            pltpu.SemaphoreType.DMA((len(FAR), 1, N_Y)),
        ],
    )

    over_core = total(keep, swapped(give, "core", lambda i: 1 - i))
    step = swapped(over_core, "x", lambda i: i ^ 1)
    over_pair = total(over_core, step)
    step = swapped(over_pair, "x", lambda i: 3 - i)
    mine = total(over_pair, step)
    other = swapped(mine, "core", lambda i: 1 - i)
    first = lax.axis_index("core") == 0
    d_inputs = jnp.concatenate(
        [jnp.where(first, mine, other), jnp.where(first, other, mine)], axis=0
    )

    by_y = exchange(dw, "y")
    over_y = by_y.astype(F32).sum(0).astype(BF)
    by_near = exchange(over_y, "zl")
    over_near = by_near.astype(F32).sum(0).astype(BF)
    to_far = jnp.broadcast_to(over_near, (2, *over_near.shape)).reshape(4, rows, h)
    by_far = exchange(to_far, ("rep", "zh"))
    return (d_inputs, by_far.astype(F32).sum(0))


def solution(mesh):
    split = Mesh(
        mesh.devices.reshape(2, 2, 4, N_Y, 4, 2),
        ("rep", "zh", "zl", "y", "x", "core"),
    )
    placed = (P(REP_FS, None), P(FS, TP), P(TP, FS), P(REP_FS, None))
    return jax.shard_map(
        per_device,
        mesh=split,
        in_specs=placed,
        out_specs=(P(REP_FS, None), P(FS, TP)),
        check_vma=False,
    )
```

```python
import jax
import jax.numpy as jnp
from jax import lax
from jax.experimental import pallas as pl
from jax.experimental.pallas import tpu as pltpu
from jax.sharding import Mesh
from jax.sharding import PartitionSpec as P


FS = ("zh", "zl", "y")
REP_FS = ("rep", "zh", "zl", "y")
Z = ("rep", "zh", "zl")
TP = ("x", "core")
N_Z = 8
N_Y = 4

BF = jnp.bfloat16
F32 = jnp.float32
NEAR = (0, 1, -1)
FAR = (2, -2, 3, -3, 4)


def exchange(parts, axes):
    return lax.all_to_all(parts, axes, split_axis=0, concat_axis=0, tiled=True)


def copies_over(value, axes):
    n = lax.axis_size(axes)
    copies = jnp.broadcast_to(value, (n, *value.shape))
    return exchange(copies, axes)


def shifted(value, axes, step):
    n = lax.axis_size(axes)
    return lax.ppermute(value, axes, [(i, (i + step) % n) for i in range(n)])


def swapped(value, axes, partner):
    n = lax.axis_size(axes)
    return lax.ppermute(value, axes, [(i, partner(i)) for i in range(n)])


def z_blocks(*groups):
    me = lax.axis_index("zh") * 4 + lax.axis_index("zl")
    for ref, shifts in groups:
        for k, shift in enumerate(shifts):
            yield ref, k, lax.rem(me - shift + 2 * N_Z, N_Z)


def rows_of(ref, k, part):
    rows = ref.shape[2] // 2
    at = slice(part * rows, (part + 1) * rows)
    return jnp.concatenate([ref[y, k, at] for y in range(N_Y)], axis=0)


def add_products(x_ref, c_ref, ref, shifts, pre_acc, hid_acc, fresh):
    width = N_Y * ref.shape[2] // 2
    for ref, k, z in z_blocks((ref, shifts)):
        at = pl.ds(pl.multiple_of(z * width, width), width)
        pre = jnp.dot(x_ref[:, at], rows_of(ref, k, 0), preferred_element_type=F32)
        hid = jnp.dot(c_ref[:, at], rows_of(ref, k, 1), preferred_element_type=F32)
        if fresh and k == 0:
            pre_acc[...] = pre
            hid_acc[...] = hid
        else:
            pre_acc[...] += pre
            hid_acc[...] += hid


def near_kernel(x_ref, c_ref, near_ref, pre_ref, hid_ref):
    add_products(x_ref, c_ref, near_ref, NEAR, pre_ref, hid_ref, True)


def far_copies(plus, minus, dsts, sems):
    me = lax.axis_index("y")
    rows = plus[0].shape[0] // 5
    width = N_Y * rows
    copies = []
    for n in range(len(FAR)):
        group = []
        for part, dst in enumerate(dsts):
            if n < 4:
                refs, piece = (plus, minus)[n % 2], n // 2 * 2 + part
            else:
                refs, piece = (plus, minus)[part], 4
            for k, dist in enumerate((0, 1, -1, 2)):
                y = lax.rem(me - dist + 2 * N_Y, N_Y)
                at = pl.multiple_of(n * width + y * rows, rows)
                copy = pltpu.make_async_copy(
                    refs[k].at[pl.ds(piece * rows, rows)],
                    dst.at[pl.ds(at, rows)],
                    sems.at[n, part, k],
                )
                copy.start()
                group.append(copy)
        copies.append(group)
    return copies


def weight_kernel(x_ref, c_ref, pre_ref, hid_ref, *refs):
    plus, minus = refs[0:4], refs[4:8]
    grad_hbm, dw_hbm, up, down, pre_acc, hid_acc, grad, dw, far_sems, out_sems = refs[8:]
    width = dw.shape[1] * dw.shape[2]
    blocks = far_copies(plus, minus, (up, down), far_sems)
    for n, (_, _, z) in enumerate(z_blocks((None, FAR))):
        for copy in blocks[n]:
            copy.wait()
        at = pl.ds(pl.multiple_of(z * width, width), width)
        mine = slice(n * width, (n + 1) * width)
        pre = jnp.dot(x_ref[:, at], up[mine], preferred_element_type=F32)
        hid = jnp.dot(c_ref[:, at], down[mine], preferred_element_type=F32)
        pre_acc[...] = (pre_ref if n == 0 else pre_acc)[...] + pre
        hid_acc[...] = (hid_ref if n == 0 else hid_acc)[...] + hid
    grad[...] = (2.0 * jnp.maximum(pre_acc[...], 0.0) * hid_acc[...]).astype(BF)
    out = [pltpu.make_async_copy(grad, grad_hbm, out_sems.at[N_Z])]
    out[0].start()
    for z in range(N_Z):
        product = lax.dot_general(
            x_ref[:, z * width : (z + 1) * width], grad[...],
            (((0,), (0,)), ((), ())), preferred_element_type=F32,
        ).astype(BF)
        dw[z] = product.reshape(dw.shape[1:])
        copy = pltpu.make_async_copy(
            dw.at[z], dw_hbm.at[:, z % 4, z // 4], out_sems.at[z]
        )
        copy.start()
        out.append(copy)
    for copy in out:
        copy.wait()


def input_kernel(grad_ref, near_ref, *refs):
    plus, minus = refs[0:4], refs[4:8]
    keep_ref, give_ref, up, sems = refs[8:]
    core = lax.axis_index("core")
    tokens = keep_ref.shape[0]
    width = N_Y * near_ref.shape[2] // 2
    copies = far_copies(plus, minus, (up,), sems)
    for group in copies:
        for copy in group:
            copy.wait()
    for out, which in ((give_ref, 1 - core), (keep_ref, core)):
        mine = grad_ref[pl.ds(pl.multiple_of(which * tokens, tokens), tokens), :]
        for ref, k, z in z_blocks((near_ref, NEAR), (None, FAR)):
            if ref is None:
                block = up[k * width : (k + 1) * width]
            else:
                block = rows_of(ref, k, 0)
            out[:, pl.ds(pl.multiple_of(z * width, width), width)] = lax.dot_general(
                mine, block, (((1,), (1,)), ((), ())), preferred_element_type=F32
            ).astype(BF)


def call(kernel, outs, args, flops, in_any, scratch=(), dtype=BF, out_hbm=()):
    vm = pl.BlockSpec(memory_space=pltpu.VMEM)
    any_ = pl.BlockSpec(memory_space=pl.ANY)
    hbm = pl.BlockSpec(memory_space=pltpu.HBM)
    return pl.pallas_call(
        kernel,
        out_shape=tuple(
            pltpu.HBM(s, dtype) if k in out_hbm else jax.ShapeDtypeStruct(s, dtype)
            for k, s in enumerate(outs)
        ),
        in_specs=[any_ if k in in_any else vm for k in range(len(args))],
        out_specs=tuple(hbm if k in out_hbm else vm for k in range(len(outs))),
        scratch_shapes=scratch,
        compiler_params=pltpu.CompilerParams(vmem_limit_bytes=24 * 2**20),
        cost_estimate=pl.CostEstimate(
            flops=flops,
            bytes_accessed=2 * sum(a.size for a in args),
            transcendentals=0,
        ),
    )(*args)


def total(a, b):
    return (a.astype(F32) + b.astype(F32)).astype(BF)


def per_device(inputs, w_up, w_down, cotangent):
    rows, h = w_up.shape
    tokens, width = inputs.shape
    own = jnp.concatenate([w_up, w_down.T], axis=0)
    back = [own]
    ahead = [own]
    for _ in range(3):
        back.append(shifted(back[-1], Z, 1))
        ahead.append(shifted(ahead[-1], Z, -1))
    plus_last = shifted(back[3][:rows], Z, 1)
    minus_last = shifted(ahead[3][rows:], Z, -1)
    near = copies_over(jnp.stack([own, back[1], ahead[1]]), "y")
    plus = [jnp.concatenate([back[2], back[3], plus_last], axis=0)]
    minus = [jnp.concatenate([ahead[2], ahead[3], minus_last], axis=0)]
    plus.append(shifted(plus[0], "y", 1))
    minus_after = shifted(minus[0], "y", -1)
    minus.append(shifted(minus[0], "y", 1))
    plus.append(shifted(plus[0], "y", -1))
    minus.append(minus_after)
    plus.append(shifted(plus[1], "y", 1))
    minus.append(shifted(minus_after, "y", -1))
    unit = tokens * width * h // 2
    part = N_Y * rows
    pre, hid = call(
        near_kernel,
        [(tokens, h)] * 2,
        (inputs, cotangent, near),
        3 * unit,
        (),
        dtype=F32,
    )
    grad, dw = call(
        weight_kernel,
        [(tokens, h), (N_Y, 4, 2, rows, h)],
        (inputs, cotangent, pre, hid, *plus, *minus),
        9 * unit,
        range(4, 12),
        [
            pltpu.VMEM((len(FAR) * part, h), BF),
            pltpu.VMEM((len(FAR) * part, h), BF),
            pltpu.VMEM((tokens, h), F32),
            pltpu.VMEM((tokens, h), F32),
            pltpu.VMEM((tokens, h), BF),
            pltpu.VMEM((N_Z, N_Y, rows, h), BF),
            pltpu.SemaphoreType.DMA((len(FAR), 2, N_Y)),
            pltpu.SemaphoreType.DMA((N_Z + 1,)),
        ],
        out_hbm=(0, 1),
    )
    keep, give = call(
        input_kernel,
        [(tokens // 2, width)] * 2,
        (grad, near, *plus, *minus),
        4 * unit,
        range(2, 10),
        [
            pltpu.VMEM((len(FAR) * part, h), BF),
            pltpu.SemaphoreType.DMA((len(FAR), 1, N_Y)),
        ],
    )

    over_core = total(keep, swapped(give, "core", lambda i: 1 - i))
    step = swapped(over_core, "x", lambda i: i ^ 1)
    over_pair = total(over_core, step)
    step = swapped(over_pair, "x", lambda i: 3 - i)
    mine = total(over_pair, step)
    other = swapped(mine, "core", lambda i: 1 - i)
    first = lax.axis_index("core") == 0
    d_inputs = jnp.concatenate(
        [jnp.where(first, mine, other), jnp.where(first, other, mine)], axis=0
    )

    by_y = exchange(dw, "y")
    over_y = by_y.astype(F32).sum(0).astype(BF)
    by_near = exchange(over_y, "zl")
    over_near = by_near.astype(F32).sum(0).astype(BF)
    to_far = jnp.broadcast_to(over_near, (2, *over_near.shape)).reshape(4, rows, h)
    by_far = exchange(to_far, ("rep", "zh"))
    return (d_inputs, by_far.astype(F32).sum(0))


def solution(mesh):
    split = Mesh(
        mesh.devices.reshape(2, 2, 4, N_Y, 4, 2),
        ("rep", "zh", "zl", "y", "x", "core"),
    )
    placed = (P(REP_FS, None), P(FS, TP), P(TP, FS), P(REP_FS, None))
    return jax.shard_map(
        per_device,
        mesh=split,
        in_specs=placed,
        out_specs=(P(REP_FS, None), P(FS, TP)),
        check_vma=False,
    )
```

```python
import jax
import jax.numpy as jnp
from jax import lax
from jax.experimental import pallas as pl
from jax.experimental.pallas import tpu as pltpu
from jax.sharding import Mesh
from jax.sharding import PartitionSpec as P


FS = ("zh", "zl", "y")
REP_FS = ("rep", "zh", "zl", "y")
Z = ("rep", "zh", "zl")
TP = ("x", "core")
N_Z = 8
N_Y = 4

BF = jnp.bfloat16
F32 = jnp.float32
NEAR = (0, 1, -1)
FAR = (2, -2, 3, -3, 4)


def exchange(parts, axes):
    return lax.all_to_all(parts, axes, split_axis=0, concat_axis=0, tiled=True)


def copies_over(value, axes):
    n = lax.axis_size(axes)
    copies = jnp.broadcast_to(value, (n, *value.shape))
    return exchange(copies, axes)


def shifted(value, axes, step):
    n = lax.axis_size(axes)
    return lax.ppermute(value, axes, [(i, (i + step) % n) for i in range(n)])


def swapped(value, axes, partner):
    n = lax.axis_size(axes)
    return lax.ppermute(value, axes, [(i, partner(i)) for i in range(n)])


def z_blocks(*groups):
    me = lax.axis_index("zh") * 4 + lax.axis_index("zl")
    for ref, shifts in groups:
        for k, shift in enumerate(shifts):
            yield ref, k, lax.rem(me - shift + 2 * N_Z, N_Z)


def rows_of(ref, k, part):
    rows = ref.shape[2] // 2
    at = slice(part * rows, (part + 1) * rows)
    return jnp.concatenate([ref[y, k, at] for y in range(N_Y)], axis=0)


def near_kernel(x_hbm, c_hbm, near_ref, pre_ref, hid_ref, x_ref, c_ref, sems):
    width = N_Y * near_ref.shape[2] // 2
    groups = (near_ref, NEAR), (None, FAR)
    places = [
        pl.ds(pl.multiple_of(z * width, width), width) for _, _, z in z_blocks(*groups)
    ]
    copies = [
        [
            pltpu.make_async_copy(src.at[:, at], dst.at[:, at], sems.at[n, part])
            for part, (src, dst) in enumerate(((x_hbm, x_ref), (c_hbm, c_ref)))
        ]
        for n, at in enumerate(places)
    ]
    for pair in copies:
        for copy in pair:
            copy.start()
    for n, at in enumerate(places):
        for copy in copies[n]:
            copy.wait()
        if n >= len(NEAR):
            continue
        up, down = rows_of(near_ref, n, 0), rows_of(near_ref, n, 1)
        pre = jnp.dot(x_ref[:, at], up, preferred_element_type=F32)
        hid = jnp.dot(c_ref[:, at], down, preferred_element_type=F32)
        if n == 0:
            pre_ref[...] = pre
            hid_ref[...] = hid
        else:
            pre_ref[...] += pre
            hid_ref[...] += hid


def far_copies(plus, minus, dsts, sems):
    me = lax.axis_index("y")
    rows = plus[0].shape[0] // 5
    width = N_Y * rows
    copies = []
    for n in range(len(FAR)):
        group = []
        for part, dst in enumerate(dsts):
            if n < 4:
                refs, piece = (plus, minus)[n % 2], n // 2 * 2 + part
            else:
                refs, piece = (plus, minus)[part], 4
            for k, dist in enumerate((0, 1, -1, 2)):
                y = lax.rem(me - dist + 2 * N_Y, N_Y)
                at = pl.multiple_of(n * width + y * rows, rows)
                copy = pltpu.make_async_copy(
                    refs[k].at[pl.ds(piece * rows, rows)],
                    dst.at[pl.ds(at, rows)],
                    sems.at[n, part, k],
                )
                copy.start()
                group.append(copy)
        copies.append(group)
    return copies


def weight_kernel(x_ref, c_ref, pre_ref, hid_ref, *refs):
    plus, minus = refs[0:4], refs[4:8]
    grad_hbm, dw_hbm, up, down, pre_acc, hid_acc, grad, dw, far_sems, out_sems = refs[8:]
    width = dw.shape[1] * dw.shape[2]
    blocks = far_copies(plus, minus, (up, down), far_sems)
    for n, (_, _, z) in enumerate(z_blocks((None, FAR))):
        for copy in blocks[n]:
            copy.wait()
        at = pl.ds(pl.multiple_of(z * width, width), width)
        mine = slice(n * width, (n + 1) * width)
        pre = jnp.dot(x_ref[:, at], up[mine], preferred_element_type=F32)
        hid = jnp.dot(c_ref[:, at], down[mine], preferred_element_type=F32)
        pre_acc[...] = (pre_ref if n == 0 else pre_acc)[...] + pre
        hid_acc[...] = (hid_ref if n == 0 else hid_acc)[...] + hid
    grad[...] = (2.0 * jnp.maximum(pre_acc[...], 0.0) * hid_acc[...]).astype(BF)
    out = [pltpu.make_async_copy(grad, grad_hbm, out_sems.at[N_Z])]
    out[0].start()
    for z in range(N_Z):
        product = lax.dot_general(
            x_ref[:, z * width : (z + 1) * width], grad[...],
            (((0,), (0,)), ((), ())), preferred_element_type=F32,
        ).astype(BF)
        dw[z] = product.reshape(dw.shape[1:])
        copy = pltpu.make_async_copy(
            dw.at[z], dw_hbm.at[:, z % 4, z // 4], out_sems.at[z]
        )
        copy.start()
        out.append(copy)
    for copy in out:
        copy.wait()


def input_kernel(grad_ref, near_ref, *refs):
    plus, minus = refs[0:4], refs[4:8]
    keep_ref, give_ref, up, sems = refs[8:]
    core = lax.axis_index("core")
    tokens = keep_ref.shape[0]
    width = N_Y * near_ref.shape[2] // 2
    copies = far_copies(plus, minus, (up,), sems)
    for group in copies:
        for copy in group:
            copy.wait()
    for out, which in ((give_ref, 1 - core), (keep_ref, core)):
        mine = grad_ref[pl.ds(pl.multiple_of(which * tokens, tokens), tokens), :]
        for ref, k, z in z_blocks((near_ref, NEAR), (None, FAR)):
            if ref is None:
                block = up[k * width : (k + 1) * width]
            else:
                block = rows_of(ref, k, 0)
            out[:, pl.ds(pl.multiple_of(z * width, width), width)] = lax.dot_general(
                mine, block, (((1,), (1,)), ((), ())), preferred_element_type=F32
            ).astype(BF)


def call(kernel, outs, args, flops, in_any, scratch=(), out_hbm=(), limit=24 * 2**20):
    vm = pl.BlockSpec(memory_space=pltpu.VMEM)
    any_ = pl.BlockSpec(memory_space=pl.ANY)
    hbm = pl.BlockSpec(memory_space=pltpu.HBM)
    return pl.pallas_call(
        kernel,
        out_shape=tuple(
            pltpu.HBM(s, t) if k in out_hbm else jax.ShapeDtypeStruct(s, t)
            for k, (s, t) in enumerate(outs)
        ),
        in_specs=[any_ if k in in_any else vm for k in range(len(args))],
        out_specs=tuple(hbm if k in out_hbm else vm for k in range(len(outs))),
        scratch_shapes=scratch,
        compiler_params=pltpu.CompilerParams(vmem_limit_bytes=limit),
        cost_estimate=pl.CostEstimate(
            flops=flops,
            bytes_accessed=2 * sum(a.size for a in args),
            transcendentals=0,
        ),
    )(*args)


def total(a, b):
    return (a.astype(F32) + b.astype(F32)).astype(BF)


def per_device(inputs, w_up, w_down, cotangent):
    rows, h = w_up.shape
    tokens, width = inputs.shape
    own = jnp.concatenate([w_up, w_down.T], axis=0)
    back = [own]
    ahead = [own]
    for _ in range(3):
        back.append(shifted(back[-1], Z, 1))
        ahead.append(shifted(ahead[-1], Z, -1))
    plus_last = shifted(back[3][:rows], Z, 1)
    minus_last = shifted(ahead[3][rows:], Z, -1)
    near = copies_over(jnp.stack([own, back[1], ahead[1]]), "y")
    plus = [jnp.concatenate([back[2], back[3], plus_last], axis=0)]
    minus = [jnp.concatenate([ahead[2], ahead[3], minus_last], axis=0)]
    plus.append(shifted(plus[0], "y", 1))
    minus_after = shifted(minus[0], "y", -1)
    minus.append(shifted(minus[0], "y", 1))
    plus.append(shifted(plus[0], "y", -1))
    minus.append(minus_after)
    plus.append(shifted(plus[1], "y", 1))
    minus.append(shifted(minus_after, "y", -1))
    inputs = pltpu.with_memory_space_constraint(inputs, pltpu.HBM)
    cotangent = pltpu.with_memory_space_constraint(cotangent, pltpu.HBM)
    unit = tokens * width * h // 2
    part = N_Y * rows
    pre, hid, inputs, cotangent = call(
        near_kernel,
        [((tokens, h), F32)] * 2 + [((tokens, width), BF)] * 2,
        (inputs, cotangent, near),
        3 * unit,
        (0, 1),
        [pltpu.SemaphoreType.DMA((N_Z, 2))],
    )
    grad, dw = call(
        weight_kernel,
        [((tokens, h), BF), ((N_Y, 4, 2, rows, h), BF)],
        (inputs, cotangent, pre, hid, *plus, *minus),
        9 * unit,
        range(4, 12),
        [
            pltpu.VMEM((len(FAR) * part, h), BF),
            pltpu.VMEM((len(FAR) * part, h), BF),
            pltpu.VMEM((tokens, h), F32),
            pltpu.VMEM((tokens, h), F32),
            pltpu.VMEM((tokens, h), BF),
            pltpu.VMEM((N_Z, N_Y, rows, h), BF),
            pltpu.SemaphoreType.DMA((len(FAR), 2, N_Y)),
            pltpu.SemaphoreType.DMA((N_Z + 1,)),
        ],
        out_hbm=(0, 1),
    )
    keep, give = call(
        input_kernel,
        [((tokens // 2, width), BF)] * 2,
        (grad, near, *plus, *minus),
        4 * unit,
        range(2, 10),
        [
            pltpu.VMEM((len(FAR) * part, h), BF),
            pltpu.SemaphoreType.DMA((len(FAR), 1, N_Y)),
        ],
        limit=None,
    )

    over_core = total(keep, swapped(give, "core", lambda i: 1 - i))
    step = swapped(over_core, "x", lambda i: i ^ 1)
    over_pair = total(over_core, step)
    step = swapped(over_pair, "x", lambda i: 3 - i)
    mine = total(over_pair, step)
    other = swapped(mine, "core", lambda i: 1 - i)
    first = lax.axis_index("core") == 0
    d_inputs = jnp.concatenate(
        [jnp.where(first, mine, other), jnp.where(first, other, mine)], axis=0
    )

    by_y = exchange(dw, "y")
    over_y = by_y.astype(F32).sum(0).astype(BF)
    by_near = exchange(over_y, "zl")
    over_near = by_near.astype(F32).sum(0).astype(BF)
    to_far = jnp.broadcast_to(over_near, (2, *over_near.shape)).reshape(4, rows, h)
    by_far = exchange(to_far, ("rep", "zh"))
    return (d_inputs, by_far.astype(F32).sum(0))


def solution(mesh):
    split = Mesh(
        mesh.devices.reshape(2, 2, 4, N_Y, 4, 2),
        ("rep", "zh", "zl", "y", "x", "core"),
    )
    placed = (P(REP_FS, None), P(FS, TP), P(TP, FS), P(REP_FS, None))
    return jax.shard_map(
        per_device,
        mesh=split,
        in_specs=placed,
        out_specs=(P(REP_FS, None), P(FS, TP)),
        check_vma=False,
    )
```

```python
import jax
import jax.numpy as jnp
from jax import lax
from jax.experimental import pallas as pl
from jax.experimental.pallas import tpu as pltpu
from jax.sharding import Mesh
from jax.sharding import PartitionSpec as P


FS = ("zh", "zl", "y")
REP_FS = ("rep", "zh", "zl", "y")
Z = ("rep", "zh", "zl")
TP = ("x", "core")
N_Z = 8
N_Y = 4

BF = jnp.bfloat16
F32 = jnp.float32
NEAR = (0, 1, -1)
FAR = (2, -2, 3, -3, 4)


def exchange(parts, axes):
    return lax.all_to_all(parts, axes, split_axis=0, concat_axis=0, tiled=True)


def copies_over(value, axes):
    n = lax.axis_size(axes)
    copies = jnp.broadcast_to(value, (n, *value.shape))
    return exchange(copies, axes)


def shifted(value, axes, step):
    n = lax.axis_size(axes)
    return lax.ppermute(value, axes, [(i, (i + step) % n) for i in range(n)])


def swapped(value, axes, partner):
    n = lax.axis_size(axes)
    return lax.ppermute(value, axes, [(i, partner(i)) for i in range(n)])


def z_blocks(*groups):
    me = lax.axis_index("zh") * 4 + lax.axis_index("zl")
    for ref, shifts in groups:
        for k, shift in enumerate(shifts):
            yield ref, k, lax.rem(me - shift + 2 * N_Z, N_Z)


def rows_of(ref, k, part):
    rows = ref.shape[2] // 2
    at = slice(part * rows, (part + 1) * rows)
    return jnp.concatenate([ref[y, k, at] for y in range(N_Y)], axis=0)


def near_kernel(x_hbm, c_hbm, near_ref, pre_ref, hid_ref, x_ref, c_ref, sems):
    width = N_Y * near_ref.shape[2] // 2
    groups = (near_ref, NEAR), (None, FAR)
    places = [
        pl.ds(pl.multiple_of(z * width, width), width) for _, _, z in z_blocks(*groups)
    ]
    copies = [
        [
            pltpu.make_async_copy(src.at[:, at], dst.at[:, at], sems.at[n, part])
            for part, (src, dst) in enumerate(((x_hbm, x_ref), (c_hbm, c_ref)))
        ]
        for n, at in enumerate(places)
    ]
    for pair in copies:
        for copy in pair:
            copy.start()
    for n, at in enumerate(places):
        for copy in copies[n]:
            copy.wait()
        if n >= len(NEAR):
            continue
        up, down = rows_of(near_ref, n, 0), rows_of(near_ref, n, 1)
        pre = jnp.dot(x_ref[:, at], up, preferred_element_type=F32)
        hid = jnp.dot(c_ref[:, at], down, preferred_element_type=F32)
        if n == 0:
            pre_ref[...] = pre
            hid_ref[...] = hid
        else:
            pre_ref[...] += pre
            hid_ref[...] += hid


def order_far(plus, minus, dsts):
    me = lax.axis_index("y")
    rows = plus[0].shape[0] // 5
    for k, dist in enumerate((0, 1, -1, 2)):
        y = lax.rem(me - dist + 2 * N_Y, N_Y)
        for n in range(len(FAR)):
            for part, dst in enumerate(dsts):
                if n < 4:
                    ref, piece = (plus, minus)[n % 2][k], n // 2 * 2 + part
                else:
                    ref, piece = (plus, minus)[part][k], 4
                at = pl.multiple_of(n * N_Y * rows + y * rows, rows)
                dst[pl.ds(at, rows), :] = ref[piece * rows : (piece + 1) * rows, :]


def weight_kernel(x_ref, c_ref, pre_ref, hid_ref, *refs):
    plus, minus = refs[0:4], refs[4:8]
    grad_hbm, dw_hbm, up_hbm, up, down, pre_acc, hid_acc, grad, dw, out_sems = refs[8:]
    width = dw.shape[1] * dw.shape[2]
    order_far(plus, minus, (up, down))
    out = [pltpu.make_async_copy(up, up_hbm, out_sems.at[N_Z + 1])]
    out[0].start()
    for n, (_, _, z) in enumerate(z_blocks((None, FAR))):
        at = pl.ds(pl.multiple_of(z * width, width), width)
        mine = slice(n * width, (n + 1) * width)
        pre = jnp.dot(x_ref[:, at], up[mine], preferred_element_type=F32)
        hid = jnp.dot(c_ref[:, at], down[mine], preferred_element_type=F32)
        pre_acc[...] = (pre_ref if n == 0 else pre_acc)[...] + pre
        hid_acc[...] = (hid_ref if n == 0 else hid_acc)[...] + hid
    grad[...] = (2.0 * jnp.maximum(pre_acc[...], 0.0) * hid_acc[...]).astype(BF)
    out.append(pltpu.make_async_copy(grad, grad_hbm, out_sems.at[N_Z]))
    out[1].start()
    for z in range(N_Z):
        product = lax.dot_general(
            x_ref[:, z * width : (z + 1) * width], grad[...],
            (((0,), (0,)), ((), ())), preferred_element_type=F32,
        ).astype(BF)
        dw[z] = product.reshape(dw.shape[1:])
        copy = pltpu.make_async_copy(
            dw.at[z], dw_hbm.at[:, z % 4, z // 4], out_sems.at[z]
        )
        copy.start()
        out.append(copy)
    for copy in out:
        copy.wait()


def input_kernel(grad_ref, near_ref, up_ref, keep_ref, give_ref):
    core = lax.axis_index("core")
    tokens = keep_ref.shape[0]
    width = N_Y * near_ref.shape[2] // 2
    for out, which in ((give_ref, 1 - core), (keep_ref, core)):
        mine = grad_ref[pl.ds(pl.multiple_of(which * tokens, tokens), tokens), :]
        for ref, k, z in z_blocks((near_ref, NEAR), (None, FAR)):
            if ref is None:
                block = up_ref[k * width : (k + 1) * width]
            else:
                block = rows_of(ref, k, 0)
            out[:, pl.ds(pl.multiple_of(z * width, width), width)] = lax.dot_general(
                mine, block, (((1,), (1,)), ((), ())), preferred_element_type=F32
            ).astype(BF)


def call(kernel, outs, args, flops, in_any, scratch=(), out_hbm=(), limit=24 * 2**20):
    vm = pl.BlockSpec(memory_space=pltpu.VMEM)
    any_ = pl.BlockSpec(memory_space=pl.ANY)
    hbm = pl.BlockSpec(memory_space=pltpu.HBM)
    return pl.pallas_call(
        kernel,
        out_shape=tuple(
            pltpu.HBM(s, t) if k in out_hbm else jax.ShapeDtypeStruct(s, t)
            for k, (s, t) in enumerate(outs)
        ),
        in_specs=[any_ if k in in_any else vm for k in range(len(args))],
        out_specs=tuple(hbm if k in out_hbm else vm for k in range(len(outs))),
        scratch_shapes=scratch,
        compiler_params=pltpu.CompilerParams(vmem_limit_bytes=limit),
        cost_estimate=pl.CostEstimate(
            flops=flops,
            bytes_accessed=2 * sum(a.size for a in args),
            transcendentals=0,
        ),
    )(*args)


def total(a, b):
    return (a.astype(F32) + b.astype(F32)).astype(BF)


def per_device(inputs, w_up, w_down, cotangent):
    rows, h = w_up.shape
    tokens, width = inputs.shape
    own = jnp.concatenate([w_up, w_down.T], axis=0)
    back = [own]
    ahead = [own]
    for _ in range(3):
        back.append(shifted(back[-1], Z, 1))
        ahead.append(shifted(ahead[-1], Z, -1))
    plus_last = shifted(back[3][:rows], Z, 1)
    minus_last = shifted(ahead[3][rows:], Z, -1)
    near = copies_over(jnp.stack([own, back[1], ahead[1]]), "y")
    plus = [jnp.concatenate([back[2], back[3], plus_last], axis=0)]
    minus = [jnp.concatenate([ahead[2], ahead[3], minus_last], axis=0)]
    plus.append(shifted(plus[0], "y", 1))
    minus_after = shifted(minus[0], "y", -1)
    minus.append(shifted(minus[0], "y", 1))
    plus.append(shifted(plus[0], "y", -1))
    minus.append(minus_after)
    plus.append(shifted(plus[1], "y", 1))
    minus.append(shifted(minus_after, "y", -1))
    inputs = pltpu.with_memory_space_constraint(inputs, pltpu.HBM)
    cotangent = pltpu.with_memory_space_constraint(cotangent, pltpu.HBM)
    unit = tokens * width * h // 2
    part = N_Y * rows
    pre, hid, inputs, cotangent = call(
        near_kernel,
        [((tokens, h), F32)] * 2 + [((tokens, width), BF)] * 2,
        (inputs, cotangent, near),
        3 * unit,
        (0, 1),
        [pltpu.SemaphoreType.DMA((N_Z, 2))],
    )
    grad, dw, up = call(
        weight_kernel,
        [
            ((tokens, h), BF),
            ((N_Y, 4, 2, rows, h), BF),
            ((len(FAR) * part, h), BF),
        ],
        (inputs, cotangent, pre, hid, *plus, *minus),
        9 * unit,
        (),
        [
            pltpu.VMEM((len(FAR) * part, h), BF),
            pltpu.VMEM((len(FAR) * part, h), BF),
            pltpu.VMEM((tokens, h), F32),
            pltpu.VMEM((tokens, h), F32),
            pltpu.VMEM((tokens, h), BF),
            pltpu.VMEM((N_Z, N_Y, rows, h), BF),
            pltpu.SemaphoreType.DMA((N_Z + 2,)),
        ],
        out_hbm=(0, 1, 2),
    )
    keep, give = call(
        input_kernel,
        [((tokens // 2, width), BF)] * 2,
        (grad, near, up),
        4 * unit,
        (),
        limit=None,
    )

    over_core = total(keep, swapped(give, "core", lambda i: 1 - i))
    step = swapped(over_core, "x", lambda i: i ^ 1)
    over_pair = total(over_core, step)
    step = swapped(over_pair, "x", lambda i: 3 - i)
    mine = total(over_pair, step)
    other = swapped(mine, "core", lambda i: 1 - i)
    first = lax.axis_index("core") == 0
    d_inputs = jnp.concatenate(
        [jnp.where(first, mine, other), jnp.where(first, other, mine)], axis=0
    )

    by_y = exchange(dw, "y")
    over_y = by_y.astype(F32).sum(0).astype(BF)
    by_near = exchange(over_y, "zl")
    over_near = by_near.astype(F32).sum(0).astype(BF)
    to_far = jnp.broadcast_to(over_near, (2, *over_near.shape)).reshape(4, rows, h)
    by_far = exchange(to_far, ("rep", "zh"))
    return (d_inputs, by_far.astype(F32).sum(0))


def solution(mesh):
    split = Mesh(
        mesh.devices.reshape(2, 2, 4, N_Y, 4, 2),
        ("rep", "zh", "zl", "y", "x", "core"),
    )
    placed = (P(REP_FS, None), P(FS, TP), P(TP, FS), P(REP_FS, None))
    return jax.shard_map(
        per_device,
        mesh=split,
        in_specs=placed,
        out_specs=(P(REP_FS, None), P(FS, TP)),
        check_vma=False,
    )
```

```python
import jax
import jax.numpy as jnp
from jax import lax
from jax.experimental import pallas as pl
from jax.experimental.pallas import tpu as pltpu
from jax.sharding import Mesh
from jax.sharding import PartitionSpec as P


FS = ("zh", "zl", "y")
REP_FS = ("rep", "zh", "zl", "y")
Z = ("rep", "zh", "zl")
TP = ("x", "core")
N_Z = 8
N_Y = 4

BF = jnp.bfloat16
F32 = jnp.float32
NEAR = (0, 1, -1)
FAR = (2, -2, 3, -3, 4)


def exchange(parts, axes):
    return lax.all_to_all(parts, axes, split_axis=0, concat_axis=0, tiled=True)


def copies_over(value, axes):
    n = lax.axis_size(axes)
    copies = jnp.broadcast_to(value, (n, *value.shape))
    return exchange(copies, axes)


def shifted(value, axes, step):
    n = lax.axis_size(axes)
    return lax.ppermute(value, axes, [(i, (i + step) % n) for i in range(n)])


def swapped(value, axes, partner):
    n = lax.axis_size(axes)
    return lax.ppermute(value, axes, [(i, partner(i)) for i in range(n)])


def z_blocks(*groups):
    me = lax.axis_index("zh") * 4 + lax.axis_index("zl")
    for ref, shifts in groups:
        for k, shift in enumerate(shifts):
            yield ref, k, lax.rem(me - shift + 2 * N_Z, N_Z)


def rows_of(ref, k, part):
    rows = ref.shape[2] // 2
    at = slice(part * rows, (part + 1) * rows)
    return jnp.concatenate([ref[y, k, at] for y in range(N_Y)], axis=0)


def near_kernel(x_hbm, c_hbm, near_ref, pre_ref, hid_ref, x_ref, c_ref, sems):
    width = N_Y * near_ref.shape[2] // 2
    groups = (near_ref, NEAR), (None, FAR)
    places = [
        pl.ds(pl.multiple_of(z * width, width), width) for _, _, z in z_blocks(*groups)
    ]
    copies = [
        [
            pltpu.make_async_copy(src.at[:, at], dst.at[:, at], sems.at[n, part])
            for part, (src, dst) in enumerate(((x_hbm, x_ref), (c_hbm, c_ref)))
        ]
        for n, at in enumerate(places)
    ]
    for pair in copies:
        for copy in pair:
            copy.start()
    for n, at in enumerate(places):
        for copy in copies[n]:
            copy.wait()
        if n >= len(NEAR):
            continue
        up, down = rows_of(near_ref, n, 0), rows_of(near_ref, n, 1)
        pre = jnp.dot(x_ref[:, at], up, preferred_element_type=F32)
        hid = jnp.dot(c_ref[:, at], down, preferred_element_type=F32)
        if n == 0:
            pre_ref[...] = pre
            hid_ref[...] = hid
        else:
            pre_ref[...] += pre
            hid_ref[...] += hid


def order_far(plus, minus, dsts):
    me = lax.axis_index("y")
    rows = plus[0].shape[0] // 5
    for k, dist in enumerate((0, 1, -1, 2)):
        y = lax.rem(me - dist + 2 * N_Y, N_Y)
        for n in range(len(FAR)):
            for part, dst in enumerate(dsts):
                if n < 4:
                    ref, piece = (plus, minus)[n % 2][k], n // 2 * 2 + part
                else:
                    ref, piece = (plus, minus)[part][k], 4
                at = pl.multiple_of(n * N_Y * rows + y * rows, rows)
                dst[pl.ds(at, rows), :] = ref[piece * rows : (piece + 1) * rows, :]


def weight_kernel(x_ref, c_ref, pre_ref, hid_ref, *refs):
    plus, minus = refs[0:4], refs[4:8]
    grad_hbm, dw_hbm, up_hbm, up, down, pre_acc, hid_acc, grad, dw, out_sems = refs[8:]
    width = dw.shape[1] * dw.shape[2]
    order_far(plus, minus, (up, down))
    out = [pltpu.make_async_copy(up, up_hbm, out_sems.at[N_Z + 1])]
    out[0].start()
    for n, (_, _, z) in enumerate(z_blocks((None, FAR))):
        at = pl.ds(pl.multiple_of(z * width, width), width)
        mine = slice(n * width, (n + 1) * width)
        pre = jnp.dot(x_ref[:, at], up[mine], preferred_element_type=F32)
        hid = jnp.dot(c_ref[:, at], down[mine], preferred_element_type=F32)
        pre_acc[...] = (pre_ref if n == 0 else pre_acc)[...] + pre
        hid_acc[...] = (hid_ref if n == 0 else hid_acc)[...] + hid
    grad[...] = (2.0 * jnp.maximum(pre_acc[...], 0.0) * hid_acc[...]).astype(BF)
    out.append(pltpu.make_async_copy(grad, grad_hbm, out_sems.at[N_Z]))
    out[1].start()
    for z in range(N_Z):
        product = lax.dot_general(
            x_ref[:, z * width : (z + 1) * width], grad[...],
            (((0,), (0,)), ((), ())), preferred_element_type=F32,
        ).astype(BF)
        dw[z] = product.reshape(dw.shape[1:])
        copy = pltpu.make_async_copy(
            dw.at[z], dw_hbm.at[:, z % 4, z // 4], out_sems.at[z]
        )
        copy.start()
        out.append(copy)
    for copy in out:
        copy.wait()


def input_kernel(grad_ref, near_ref, up_ref, keep_ref, give_ref):
    core = lax.axis_index("core")
    tokens = keep_ref.shape[0]
    width = N_Y * near_ref.shape[2] // 2
    for out, which in ((give_ref, 1 - core), (keep_ref, core)):
        mine = grad_ref[pl.ds(pl.multiple_of(which * tokens, tokens), tokens), :]
        for ref, k, z in z_blocks((near_ref, NEAR), (None, FAR)):
            if ref is None:
                block = up_ref[k * width : (k + 1) * width]
            else:
                block = rows_of(ref, k, 0)
            out[:, pl.ds(pl.multiple_of(z * width, width), width)] = lax.dot_general(
                mine, block, (((1,), (1,)), ((), ())), preferred_element_type=F32
            ).astype(BF)


def call(kernel, outs, args, flops, in_any, scratch=(), out_hbm=(), limit=24 * 2**20):
    vm = pl.BlockSpec(memory_space=pltpu.VMEM)
    any_ = pl.BlockSpec(memory_space=pl.ANY)
    hbm = pl.BlockSpec(memory_space=pltpu.HBM)
    return pl.pallas_call(
        kernel,
        out_shape=tuple(
            pltpu.HBM(s, t) if k in out_hbm else jax.ShapeDtypeStruct(s, t)
            for k, (s, t) in enumerate(outs)
        ),
        in_specs=[any_ if k in in_any else vm for k in range(len(args))],
        out_specs=tuple(hbm if k in out_hbm else vm for k in range(len(outs))),
        scratch_shapes=scratch,
        compiler_params=pltpu.CompilerParams(vmem_limit_bytes=limit),
        cost_estimate=pl.CostEstimate(
            flops=flops,
            bytes_accessed=2 * sum(a.size for a in args),
            transcendentals=0,
        ),
    )(*args)


def total(a, b):
    return (a.astype(F32) + b.astype(F32)).astype(BF)


def per_device(inputs, w_up, w_down, cotangent):
    rows, h = w_up.shape
    tokens, width = inputs.shape
    own = jnp.concatenate([w_up, w_down.T], axis=0)
    back = [own]
    ahead = [own]
    for _ in range(3):
        ahead.append(shifted(ahead[-1], Z, -1))
        back.append(shifted(back[-1], Z, 1))
    last = shifted(back[3], Z, 1)
    plus_last, minus_last = last[:rows], last[rows:]
    near = jnp.stack([own, back[1], ahead[1]])
    near = copies_over(near, "y")
    plus = [jnp.concatenate([back[2], back[3], plus_last], axis=0)]
    minus = [jnp.concatenate([ahead[2], ahead[3], minus_last], axis=0)]
    plus.append(shifted(plus[0], "y", 1))
    minus_after = shifted(minus[0], "y", -1)
    minus.append(shifted(minus[0], "y", 1))
    plus.append(shifted(plus[0], "y", -1))
    minus.append(minus_after)
    plus.append(shifted(plus[1], "y", 1))
    minus.append(shifted(minus_after, "y", -1))
    inputs = pltpu.with_memory_space_constraint(inputs, pltpu.HBM)
    cotangent = pltpu.with_memory_space_constraint(cotangent, pltpu.HBM)
    unit = tokens * width * h // 2
    part = N_Y * rows
    pre, hid, inputs, cotangent = call(
        near_kernel,
        [((tokens, h), F32)] * 2 + [((tokens, width), BF)] * 2,
        (inputs, cotangent, near),
        3 * unit,
        (0, 1),
        [pltpu.SemaphoreType.DMA((N_Z, 2))],
    )
    grad, dw, up = call(
        weight_kernel,
        [
            ((tokens, h), BF),
            ((N_Y, 4, 2, rows, h), BF),
            ((len(FAR) * part, h), BF),
        ],
        (inputs, cotangent, pre, hid, *plus, *minus),
        9 * unit,
        (),
        [
            pltpu.VMEM((len(FAR) * part, h), BF),
            pltpu.VMEM((len(FAR) * part, h), BF),
            pltpu.VMEM((tokens, h), F32),
            pltpu.VMEM((tokens, h), F32),
            pltpu.VMEM((tokens, h), BF),
            pltpu.VMEM((N_Z, N_Y, rows, h), BF),
            pltpu.SemaphoreType.DMA((N_Z + 2,)),
        ],
        out_hbm=(0, 1, 2),
    )
    keep, give = call(
        input_kernel,
        [((tokens // 2, width), BF)] * 2,
        (grad, near, up),
        4 * unit,
        (),
        limit=None,
    )

    over_core = total(keep, swapped(give, "core", lambda i: 1 - i))
    step = swapped(over_core, "x", lambda i: i ^ 1)
    over_pair = total(over_core, step)
    step = swapped(over_pair, "x", lambda i: 3 - i)
    mine = total(over_pair, step)
    other = swapped(mine, "core", lambda i: 1 - i)
    first = lax.axis_index("core") == 0
    d_inputs = jnp.concatenate(
        [jnp.where(first, mine, other), jnp.where(first, other, mine)], axis=0
    )

    by_y = exchange(dw, "y")
    over_y = by_y.astype(F32).sum(0).astype(BF)
    by_near = exchange(over_y, "zl")
    over_near = by_near.astype(F32).sum(0).astype(BF)
    to_far = jnp.broadcast_to(over_near, (2, *over_near.shape)).reshape(4, rows, h)
    by_far = exchange(to_far, ("rep", "zh"))
    return (d_inputs, by_far.astype(F32).sum(0))


def solution(mesh):
    split = Mesh(
        mesh.devices.reshape(2, 2, 4, N_Y, 4, 2),
        ("rep", "zh", "zl", "y", "x", "core"),
    )
    placed = (P(REP_FS, None), P(FS, TP), P(TP, FS), P(REP_FS, None))
    return jax.shard_map(
        per_device,
        mesh=split,
        in_specs=placed,
        out_specs=(P(REP_FS, None), P(FS, TP)),
        check_vma=False,
    )
```

```python
import jax
import jax.numpy as jnp
from jax import lax
from jax.experimental import pallas as pl
from jax.experimental.pallas import tpu as pltpu
from jax.sharding import Mesh
from jax.sharding import PartitionSpec as P


FS = ("zh", "zl", "y")
REP_FS = ("rep", "zh", "zl", "y")
Z = ("rep", "zh", "zl")
TP = ("x", "core")
N_Z = 8
N_Y = 4

BF = jnp.bfloat16
F32 = jnp.float32
NEAR = (0, 1, -1)
FAR = (2, -2, 3, -3, 4)


def exchange(parts, axes):
    return lax.all_to_all(parts, axes, split_axis=0, concat_axis=0, tiled=True)


def copies_over(value, axes):
    n = lax.axis_size(axes)
    copies = jnp.broadcast_to(value, (n, *value.shape))
    return exchange(copies, axes)


def shifted(value, axes, step):
    n = lax.axis_size(axes)
    return lax.ppermute(value, axes, [(i, (i + step) % n) for i in range(n)])


def swapped(value, axes, partner):
    n = lax.axis_size(axes)
    return lax.ppermute(value, axes, [(i, partner(i)) for i in range(n)])


def z_blocks(*groups):
    me = lax.axis_index("zh") * 4 + lax.axis_index("zl")
    for ref, shifts in groups:
        for k, shift in enumerate(shifts):
            yield ref, k, lax.rem(me - shift + 2 * N_Z, N_Z)


def rows_of(ref, k, part):
    rows = ref.shape[2] // 2
    at = slice(part * rows, (part + 1) * rows)
    return jnp.concatenate([ref[y, k, at] for y in range(N_Y)], axis=0)


def near_kernel(x_hbm, c_hbm, near_ref, pre_ref, hid_ref, x_ref, c_ref, sems):
    width = N_Y * near_ref.shape[2] // 2
    groups = (near_ref, NEAR), (None, FAR)
    places = [
        pl.ds(pl.multiple_of(z * width, width), width) for _, _, z in z_blocks(*groups)
    ]
    copies = [
        [
            pltpu.make_async_copy(src.at[:, at], dst.at[:, at], sems.at[n, part])
            for part, (src, dst) in enumerate(((x_hbm, x_ref), (c_hbm, c_ref)))
        ]
        for n, at in enumerate(places)
    ]
    for pair in copies:
        for copy in pair:
            copy.start()
    for n, at in enumerate(places):
        for copy in copies[n]:
            copy.wait()
        if n >= len(NEAR):
            continue
        up, down = rows_of(near_ref, n, 0), rows_of(near_ref, n, 1)
        pre = jnp.dot(x_ref[:, at], up, preferred_element_type=F32)
        hid = jnp.dot(c_ref[:, at], down, preferred_element_type=F32)
        if n == 0:
            pre_ref[...] = pre
            hid_ref[...] = hid
        else:
            pre_ref[...] += pre
            hid_ref[...] += hid


def order_far(plus, minus, dsts):
    me = lax.axis_index("y")
    rows = minus[0].shape[0] // 4
    for k, dist in enumerate((0, 1, -1, 2)):
        y = lax.rem(me - dist + 2 * N_Y, N_Y)
        for n in range(len(FAR)):
            for part, dst in enumerate(dsts):
                ref, piece = (plus, minus)[n % 2][k], n // 2 * 2 + part
                at = pl.multiple_of(n * N_Y * rows + y * rows, rows)
                dst[pl.ds(at, rows), :] = ref[piece * rows : (piece + 1) * rows, :]


def weight_kernel(x_ref, c_ref, pre_ref, hid_ref, *refs):
    plus, minus = refs[0:4], refs[4:8]
    grad_hbm, dw_hbm, up_hbm, up, down, pre_acc, hid_acc, grad, dw, out_sems = refs[8:]
    width = dw.shape[1] * dw.shape[2]
    order_far(plus, minus, (up, down))
    out = [pltpu.make_async_copy(up, up_hbm, out_sems.at[N_Z + 1])]
    out[0].start()
    for n, (_, _, z) in enumerate(z_blocks((None, FAR))):
        at = pl.ds(pl.multiple_of(z * width, width), width)
        mine = slice(n * width, (n + 1) * width)
        pre = jnp.dot(x_ref[:, at], up[mine], preferred_element_type=F32)
        hid = jnp.dot(c_ref[:, at], down[mine], preferred_element_type=F32)
        pre_acc[...] = (pre_ref if n == 0 else pre_acc)[...] + pre
        hid_acc[...] = (hid_ref if n == 0 else hid_acc)[...] + hid
    grad[...] = (2.0 * jnp.maximum(pre_acc[...], 0.0) * hid_acc[...]).astype(BF)
    out.append(pltpu.make_async_copy(grad, grad_hbm, out_sems.at[N_Z]))
    out[1].start()
    for z in range(N_Z):
        product = lax.dot_general(
            x_ref[:, z * width : (z + 1) * width], grad[...],
            (((0,), (0,)), ((), ())), preferred_element_type=F32,
        ).astype(BF)
        dw[z] = product.reshape(dw.shape[1:])
        copy = pltpu.make_async_copy(
            dw.at[z], dw_hbm.at[:, z % 4, z // 4], out_sems.at[z]
        )
        copy.start()
        out.append(copy)
    for copy in out:
        copy.wait()


def input_kernel(grad_ref, near_ref, up_ref, keep_ref, give_ref):
    core = lax.axis_index("core")
    tokens = keep_ref.shape[0]
    width = N_Y * near_ref.shape[2] // 2
    for out, which in ((give_ref, 1 - core), (keep_ref, core)):
        mine = grad_ref[pl.ds(pl.multiple_of(which * tokens, tokens), tokens), :]
        for ref, k, z in z_blocks((near_ref, NEAR), (None, FAR)):
            if ref is None:
                block = up_ref[k * width : (k + 1) * width]
            else:
                block = rows_of(ref, k, 0)
            out[:, pl.ds(pl.multiple_of(z * width, width), width)] = lax.dot_general(
                mine, block, (((1,), (1,)), ((), ())), preferred_element_type=F32
            ).astype(BF)


def call(kernel, outs, args, flops, in_any, scratch=(), out_hbm=(), limit=24 * 2**20):
    vm = pl.BlockSpec(memory_space=pltpu.VMEM)
    any_ = pl.BlockSpec(memory_space=pl.ANY)
    hbm = pl.BlockSpec(memory_space=pltpu.HBM)
    return pl.pallas_call(
        kernel,
        out_shape=tuple(
            pltpu.HBM(s, t) if k in out_hbm else jax.ShapeDtypeStruct(s, t)
            for k, (s, t) in enumerate(outs)
        ),
        in_specs=[any_ if k in in_any else vm for k in range(len(args))],
        out_specs=tuple(hbm if k in out_hbm else vm for k in range(len(outs))),
        scratch_shapes=scratch,
        compiler_params=pltpu.CompilerParams(vmem_limit_bytes=limit),
        cost_estimate=pl.CostEstimate(
            flops=flops,
            bytes_accessed=2 * sum(a.size for a in args),
            transcendentals=0,
        ),
    )(*args)


def total(a, b):
    return (a.astype(F32) + b.astype(F32)).astype(BF)


def per_device(inputs, w_up, w_down, cotangent):
    rows, h = w_up.shape
    tokens, width = inputs.shape
    own = jnp.concatenate([w_up, w_down.T], axis=0)
    back = [own]
    ahead = [own]
    for _ in range(3):
        ahead.append(shifted(ahead[-1], Z, -1))
        back.append(shifted(back[-1], Z, 1))
    last = shifted(back[3], Z, 1)
    near = jnp.stack([own, back[1], ahead[1]])
    near = copies_over(near, "y")
    minus = [jnp.concatenate([ahead[2], ahead[3]], axis=0)]
    plus = [jnp.concatenate([back[2], back[3], last], axis=0)]
    for stack in (minus, plus):
        stack.append(shifted(stack[0], "y", 1))
        stack.append(shifted(stack[0], "y", -1))
    plus.append(shifted(plus[1], "y", 1))
    minus.append(shifted(minus[2], "y", -1))
    inputs = pltpu.with_memory_space_constraint(inputs, pltpu.HBM)
    cotangent = pltpu.with_memory_space_constraint(cotangent, pltpu.HBM)
    unit = tokens * width * h // 2
    part = N_Y * rows
    pre, hid, inputs, cotangent = call(
        near_kernel,
        [((tokens, h), F32)] * 2 + [((tokens, width), BF)] * 2,
        (inputs, cotangent, near),
        3 * unit,
        (0, 1),
        [pltpu.SemaphoreType.DMA((N_Z, 2))],
    )
    grad, dw, up = call(
        weight_kernel,
        [
            ((tokens, h), BF),
            ((N_Y, 4, 2, rows, h), BF),
            ((len(FAR) * part, h), BF),
        ],
        (inputs, cotangent, pre, hid, *plus, *minus),
        9 * unit,
        (),
        [
            pltpu.VMEM((len(FAR) * part, h), BF),
            pltpu.VMEM((len(FAR) * part, h), BF),
            pltpu.VMEM((tokens, h), F32),
            pltpu.VMEM((tokens, h), F32),
            pltpu.VMEM((tokens, h), BF),
            pltpu.VMEM((N_Z, N_Y, rows, h), BF),
            pltpu.SemaphoreType.DMA((N_Z + 2,)),
        ],
        out_hbm=(0, 1, 2),
    )
    keep, give = call(
        input_kernel,
        [((tokens // 2, width), BF)] * 2,
        (grad, near, up),
        4 * unit,
        (),
        limit=None,
    )

    over_core = total(keep, swapped(give, "core", lambda i: 1 - i))
    step = swapped(over_core, "x", lambda i: i ^ 1)
    over_pair = total(over_core, step)
    step = swapped(over_pair, "x", lambda i: 3 - i)
    mine = total(over_pair, step)
    other = swapped(mine, "core", lambda i: 1 - i)
    first = lax.axis_index("core") == 0
    d_inputs = jnp.concatenate(
        [jnp.where(first, mine, other), jnp.where(first, other, mine)], axis=0
    )

    by_y = exchange(dw, "y")
    over_y = by_y.astype(F32).sum(0).astype(BF)
    by_near = exchange(over_y, "zl")
    over_near = by_near.astype(F32).sum(0).astype(BF)
    to_far = jnp.broadcast_to(over_near, (2, *over_near.shape)).reshape(4, rows, h)
    by_far = exchange(to_far, ("rep", "zh"))
    return (d_inputs, by_far.astype(F32).sum(0))


def solution(mesh):
    split = Mesh(
        mesh.devices.reshape(2, 2, 4, N_Y, 4, 2),
        ("rep", "zh", "zl", "y", "x", "core"),
    )
    placed = (P(REP_FS, None), P(FS, TP), P(TP, FS), P(REP_FS, None))
    return jax.shard_map(
        per_device,
        mesh=split,
        in_specs=placed,
        out_specs=(P(REP_FS, None), P(FS, TP)),
        check_vma=False,
    )
```

```python
import jax
import jax.numpy as jnp
from jax import lax
from jax.experimental import pallas as pl
from jax.experimental.pallas import tpu as pltpu
from jax.sharding import Mesh
from jax.sharding import PartitionSpec as P


FS = ("zh", "zl", "y")
REP_FS = ("rep", "zh", "zl", "y")
Z = ("rep", "zh", "zl")
TP = ("x", "core")
N_Z = 8
N_Y = 4

BF = jnp.bfloat16
F32 = jnp.float32
NEAR = (0, 1, -1)
FAR = (2, -2, 3, -3, 4)


def exchange(parts, axes):
    return lax.all_to_all(parts, axes, split_axis=0, concat_axis=0, tiled=True)


def copies_over(value, axes):
    n = lax.axis_size(axes)
    copies = jnp.broadcast_to(value, (n, *value.shape))
    return exchange(copies, axes)


def shifted(value, axes, step):
    n = lax.axis_size(axes)
    return lax.ppermute(value, axes, [(i, (i + step) % n) for i in range(n)])


def swapped(value, axes, partner):
    n = lax.axis_size(axes)
    return lax.ppermute(value, axes, [(i, partner(i)) for i in range(n)])


def z_blocks(*groups):
    me = lax.axis_index("zh") * 4 + lax.axis_index("zl")
    for ref, shifts in groups:
        for k, shift in enumerate(shifts):
            yield ref, k, lax.rem(me - shift + 2 * N_Z, N_Z)


def rows_of(ref, k, part):
    rows = ref.shape[2] // 2
    at = slice(part * rows, (part + 1) * rows)
    return jnp.concatenate([ref[y, k, at] for y in range(N_Y)], axis=0)


def near_kernel(x_hbm, c_hbm, near_ref, pre_ref, hid_ref, x_ref, c_ref, sems):
    width = N_Y * near_ref.shape[2] // 2
    groups = (near_ref, NEAR), (None, FAR)
    places = [
        pl.ds(pl.multiple_of(z * width, width), width) for _, _, z in z_blocks(*groups)
    ]
    copies = [
        [
            pltpu.make_async_copy(src.at[:, at], dst.at[:, at], sems.at[n, part])
            for part, (src, dst) in enumerate(((x_hbm, x_ref), (c_hbm, c_ref)))
        ]
        for n, at in enumerate(places)
    ]
    for pair in copies:
        for copy in pair:
            copy.start()
    for n, at in enumerate(places):
        for copy in copies[n]:
            copy.wait()
        if n >= len(NEAR):
            continue
        up, down = rows_of(near_ref, n, 0), rows_of(near_ref, n, 1)
        pre = jnp.dot(x_ref[:, at], up, preferred_element_type=F32)
        hid = jnp.dot(c_ref[:, at], down, preferred_element_type=F32)
        if n == 0:
            pre_ref[...] = pre
            hid_ref[...] = hid
        else:
            pre_ref[...] += pre
            hid_ref[...] += hid


def order_far(plus, minus, dsts):
    me = lax.axis_index("y")
    rows = minus[0].shape[0] // 4
    for k, dist in enumerate((0, 1, -1, 2)):
        y = lax.rem(me - dist + 2 * N_Y, N_Y)
        for n in range(len(FAR)):
            for part, dst in enumerate(dsts):
                ref, piece = (plus, minus)[n % 2][k], n // 2 * 2 + part
                at = pl.multiple_of(n * N_Y * rows + y * rows, rows)
                dst[pl.ds(at, rows), :] = ref[piece * rows : (piece + 1) * rows, :]


def weight_kernel(x_ref, c_ref, pre_ref, hid_ref, *refs):
    plus, minus = refs[0:4], refs[4:8]
    grad_hbm, dw_hbm, up_hbm, up, down, pre_acc, hid_acc, grad, dw, out_sems = refs[8:]
    width = dw.shape[1] * dw.shape[2]
    order_far(plus, minus, (up, down))
    out = [pltpu.make_async_copy(up, up_hbm, out_sems.at[N_Z + 1])]
    out[0].start()
    for n, (_, _, z) in enumerate(z_blocks((None, FAR))):
        at = pl.ds(pl.multiple_of(z * width, width), width)
        mine = slice(n * width, (n + 1) * width)
        pre = jnp.dot(x_ref[:, at], up[mine], preferred_element_type=F32)
        hid = jnp.dot(c_ref[:, at], down[mine], preferred_element_type=F32)
        pre_acc[...] = (pre_ref if n == 0 else pre_acc)[...] + pre
        hid_acc[...] = (hid_ref if n == 0 else hid_acc)[...] + hid
    grad[...] = (2.0 * jnp.maximum(pre_acc[...], 0.0) * hid_acc[...]).astype(BF)
    out.append(pltpu.make_async_copy(grad, grad_hbm, out_sems.at[N_Z]))
    out[1].start()
    for z in range(N_Z):
        product = lax.dot_general(
            x_ref[:, z * width : (z + 1) * width], grad[...],
            (((0,), (0,)), ((), ())), preferred_element_type=F32,
        ).astype(BF)
        dw[z] = product.reshape(dw.shape[1:])
        copy = pltpu.make_async_copy(
            dw.at[z], dw_hbm.at[:, z % 4, z // 4], out_sems.at[z]
        )
        copy.start()
        out.append(copy)
    for copy in out:
        copy.wait()


def input_kernel(grad_ref, near_ref, up_ref, keep_ref, give_ref):
    core = lax.axis_index("core")
    tokens = keep_ref.shape[0]
    width = N_Y * near_ref.shape[2] // 2
    for out, which in ((give_ref, 1 - core), (keep_ref, core)):
        mine = grad_ref[pl.ds(pl.multiple_of(which * tokens, tokens), tokens), :]
        for ref, k, z in z_blocks((near_ref, NEAR), (None, FAR)):
            if ref is None:
                block = up_ref[k * width : (k + 1) * width]
            else:
                block = rows_of(ref, k, 0)
            out[:, pl.ds(pl.multiple_of(z * width, width), width)] = lax.dot_general(
                mine, block, (((1,), (1,)), ((), ())), preferred_element_type=F32
            ).astype(BF)


def call(kernel, outs, args, flops, in_any, scratch=(), out_hbm=(), limit=24 * 2**20):
    vm = pl.BlockSpec(memory_space=pltpu.VMEM)
    any_ = pl.BlockSpec(memory_space=pl.ANY)
    hbm = pl.BlockSpec(memory_space=pltpu.HBM)
    return pl.pallas_call(
        kernel,
        out_shape=tuple(
            pltpu.HBM(s, t) if k in out_hbm else jax.ShapeDtypeStruct(s, t)
            for k, (s, t) in enumerate(outs)
        ),
        in_specs=[any_ if k in in_any else vm for k in range(len(args))],
        out_specs=tuple(hbm if k in out_hbm else vm for k in range(len(outs))),
        scratch_shapes=scratch,
        compiler_params=pltpu.CompilerParams(vmem_limit_bytes=limit),
        cost_estimate=pl.CostEstimate(
            flops=flops,
            bytes_accessed=2 * sum(a.size for a in args),
            transcendentals=0,
        ),
    )(*args)


def total(a, b):
    return (a.astype(F32) + b.astype(F32)).astype(BF)


def per_device(inputs, w_up, w_down, cotangent):
    rows, h = w_up.shape
    tokens, width = inputs.shape
    own = jnp.concatenate([w_up, w_down.T], axis=0)
    back = [own]
    ahead = [own]
    for _ in range(3):
        ahead.append(shifted(ahead[-1], Z, -1))
        back.append(shifted(back[-1], Z, 1))
    last = shifted(back[3], Z, 1)
    near = jnp.stack([own, back[1], ahead[1]])
    near = copies_over(near, "y")
    minus = [jnp.concatenate([ahead[2], ahead[3]], axis=0)]
    plus = [jnp.concatenate([back[2], back[3], last], axis=0)]
    sends = {}
    for name, stack, step in (
        ("minus_after", minus, -1),
        ("plus_before", plus, 1),
        ("plus_after", plus, -1),
        ("minus_before", minus, 1),
    ):
        sends[name] = shifted(stack[0], "y", step)
    minus += [sends["minus_before"], sends["minus_after"]]
    plus += [sends["plus_before"], sends["plus_after"]]
    plus.append(shifted(plus[1], "y", 1))
    minus.append(shifted(minus[2], "y", -1))
    inputs = pltpu.with_memory_space_constraint(inputs, pltpu.HBM)
    cotangent = pltpu.with_memory_space_constraint(cotangent, pltpu.HBM)
    unit = tokens * width * h // 2
    part = N_Y * rows
    pre, hid, inputs, cotangent = call(
        near_kernel,
        [((tokens, h), F32)] * 2 + [((tokens, width), BF)] * 2,
        (inputs, cotangent, near),
        3 * unit,
        (0, 1),
        [pltpu.SemaphoreType.DMA((N_Z, 2))],
    )
    grad, dw, up = call(
        weight_kernel,
        [
            ((tokens, h), BF),
            ((N_Y, 4, 2, rows, h), BF),
            ((len(FAR) * part, h), BF),
        ],
        (inputs, cotangent, pre, hid, *plus, *minus),
        9 * unit,
        (),
        [
            pltpu.VMEM((len(FAR) * part, h), BF),
            pltpu.VMEM((len(FAR) * part, h), BF),
            pltpu.VMEM((tokens, h), F32),
            pltpu.VMEM((tokens, h), F32),
            pltpu.VMEM((tokens, h), BF),
            pltpu.VMEM((N_Z, N_Y, rows, h), BF),
            pltpu.SemaphoreType.DMA((N_Z + 2,)),
        ],
        out_hbm=(0, 1, 2),
    )
    keep, give = call(
        input_kernel,
        [((tokens // 2, width), BF)] * 2,
        (grad, near, up),
        4 * unit,
        (),
        limit=None,
    )

    over_core = total(keep, swapped(give, "core", lambda i: 1 - i))
    step = swapped(over_core, "x", lambda i: i ^ 1)
    over_pair = total(over_core, step)
    step = swapped(over_pair, "x", lambda i: 3 - i)
    mine = total(over_pair, step)
    other = swapped(mine, "core", lambda i: 1 - i)
    first = lax.axis_index("core") == 0
    d_inputs = jnp.concatenate(
        [jnp.where(first, mine, other), jnp.where(first, other, mine)], axis=0
    )

    by_y = exchange(dw, "y")
    over_y = by_y.astype(F32).sum(0).astype(BF)
    by_near = exchange(over_y, "zl")
    over_near = by_near.astype(F32).sum(0).astype(BF)
    to_far = jnp.broadcast_to(over_near, (2, *over_near.shape)).reshape(4, rows, h)
    by_far = exchange(to_far, ("rep", "zh"))
    return (d_inputs, by_far.astype(F32).sum(0))


def solution(mesh):
    split = Mesh(
        mesh.devices.reshape(2, 2, 4, N_Y, 4, 2),
        ("rep", "zh", "zl", "y", "x", "core"),
    )
    placed = (P(REP_FS, None), P(FS, TP), P(TP, FS), P(REP_FS, None))
    return jax.shard_map(
        per_device,
        mesh=split,
        in_specs=placed,
        out_specs=(P(REP_FS, None), P(FS, TP)),
        check_vma=False,
    )
```
